512 devices in a mesh: grp: 2 (over y), fs: 64 (over z, core), tp: 4 (over x).
Axes of the slice: x: 4, y: 2, z: 32, core: 2. Of those that a mesh axis runs over, the one named last changes fastest.
The devices are a block of a 4x8x32 slice.
Arguments:
- tokens: bfloat16 [1536, 2048], P(('grp', 'tp')), parts along dimension 0, may hold values from -6 to 6
- routes: int32 [1536, 2], P(('grp', 'tp')), parts along dimension 0, may hold values from 0 to 3, all different within a row; in each aligned block of 192 rows (0 to 191, 192 to 383, ...) at most 128 rows name the same one
- route_weight: float32 [1536, 2], P(('grp', 'tp')), parts along dimension 0, may hold values from 0.2 to 1
- norm_gain: float32 [2048], P('fs'), may hold values from 0.1 to 1.9
- gate_train: float32 [4, 2048, 5632], P('tp', 'fs'), may hold values from -0.125 to 0.125
- up_train: float32 [4, 2048, 5632], P('tp', 'fs'), may hold values from -0.125 to 0.125
- down_train: float32 [4, 5632, 2048], P('tp', None, 'fs'), may hold values from -0.21875 to 0.21875
Outputs:
- gate_serve: bfloat16 [8, 2048, 11264], P(('grp', 'tp'), None, 'fs'), parts along dimension 0
- up_serve: bfloat16 [8, 2048, 11264], P(('grp', 'tp'), None, 'fs'), parts along dimension 0
- down_serve: bfloat16 [8, 11264, 2048], P(('grp', 'tp'), 'fs'), parts along dimension 0
- mixed: bfloat16 [1536, 2048], P(('grp', 'tp'), 'fs'), parts along dimension 0
The draws below stay inside these ranges and needn't reach their ends.
There are 2 independent parts, one for each index of `grp`. The reference program is written for one: setup_inputs(seed, part) draws one part's arguments, and reference() takes and returns one part's arrays. A program takes and returns all parts, laid end to end along the dimension named above; an argument that names none is the same for every part. Nothing has to cross between parts.
Inputs may be any that keep to these rules, and one draw needn't show every extreme that they name: `routes`: each row names 2 different experts. In each aligned block of 192 rows no expert is named by more than 128 rows, a bound that some block reaches.
All inputs are finite; a program needn't handle non-finite values.
Results may differ from the reference program's by a relative error of at most 0.0087.
Values may be sent and summed in bfloat16 or wider, within the bound.
A program may use at most 64 MiB of HBM per device.

```python
import math
import jax
import jax.numpy as jnp
import numpy as np
from jax import lax

D = 2048
FF = 5632
EXPERTS = 4
TOP = 2
TOK_DEV = 192
CAP = 128
TOKENS = 768
COPIES = 2


def strengthened(values, own_key, source, target, blocks, factor):
    def block_of(axis_at):
        return (jnp.arange(values.shape[axis_at]) // (values.shape[axis_at] // blocks)).reshape((-1,) + (1,) * (values.ndim - 1 - axis_at))

    one_side = jax.random.permutation(own_key, blocks)[block_of(target)]
    other_side = (block_of(target) + blocks // 2) % blocks
    return jnp.where((block_of(source) == one_side) | (block_of(source) == other_side), factor * values, values)


def levels(key, extent, pieces, least, largest):
    loudness = 1.0
    for dim, blocks in pieces:
        draws = jax.random.uniform(jax.random.fold_in(jax.random.fold_in(key, 6), dim), (blocks,), jnp.float32, least / len(pieces), largest / len(pieces))
        loudness = loudness * jnp.repeat(jnp.exp(draws), extent[dim] // blocks).reshape((-1,) + (1,) * (len(extent) - 1 - dim))
    return loudness


def routed_block(own_key, own, number, rows, count, top, bound, lean):
    order = jax.random.permutation(own_key, count)
    packed, usual = portions_of(count, rows * top, bound, lean, True), portions_of(count, rows * top, bound, lean, False)
    places = jnp.arange(count)

    def named(lengths, turn):
        used = int((lengths > 0).sum())
        fixed = max(1, used // 4)
        moved = fixed + (places - fixed + turn * (used - fixed)) % max(1, count - fixed)
        return jnp.zeros((count,), jnp.int32).at[order[jnp.where(places < fixed, places, moved)]].set(jnp.asarray(lengths, jnp.int32))

    lengths = jnp.where(number % 4 == 0, named(packed, number // 4), named(usual, number - number // 4 - 1))
    mixed = jax.random.permutation(jax.random.fold_in(own, 3), count)
    giver, sink = mixed[0:count // 2 * 2:2], mixed[1:count // 2 * 2:2]
    slack = jnp.minimum(lengths[giver] - 1, bound - lengths[sink]) // 2
    slack = jnp.where((giver == order[0]) | (sink == order[0]) | (lengths[sink] == 0), 0, jnp.maximum(slack, 0))
    moved = jax.random.randint(jax.random.fold_in(own, 4), (count // 2,), 0, 1 << 20) % (slack + 1)
    lengths = lengths.at[giver].add(-moved).at[sink].add(moved)
    items = jnp.searchsorted(jnp.cumsum(lengths), jnp.arange(rows * top), side="right").astype(jnp.int32)
    table = items.reshape(top, rows).T
    table = table[jax.random.permutation(jax.random.fold_in(own, 1), rows)]
    turn = jax.random.randint(jax.random.fold_in(own, 2), (rows, 1), 0, top)
    return jnp.take_along_axis(table, (jnp.arange(top)[None, :] + turn) % top, axis=1)


def portions_of(amount, total, limit, slope, full):
    weights = [(1 << 20) // math.isqrt(grade ** slope) + 1 for grade in range(1, amount + 1)]
    largest = limit if full else min(limit, max(-(-total // amount), total * weights[0] // sum(weights)))
    least = 1 if total - largest >= amount - 1 else 0
    holding, rest = [largest] + [least] * (amount - 1), total - largest - least * (amount - 1)
    while rest > 0:
        movable = [i for i in range(1, amount) if holding[i] < largest] or [i for i in range(1, amount) if holding[i] < limit]
        whole, left = sum([weights[i] for i in movable]), rest
        for i in movable:
            extra = min(limit - holding[i], max(1, left * weights[i] // whole), rest)
            holding[i] = holding[i] + extra
            rest = rest - extra
    return np.array(holding)


def gaussian(key, shape, width, limit, pieces=(), kind=jnp.bfloat16):
    values = jax.random.normal(key, shape, jnp.float32) * width
    if len(pieces) > 0:
        values = levels(key, shape, pieces, -0.22, 0.18) * values
    return jnp.clip(values, min=-limit, max=limit).astype(kind)


def gaussian_with(stream_key, dims, spread, most, split, heavy, held_as=jnp.bfloat16):
    drawn = spread * jax.random.normal(stream_key, dims, jnp.float32)
    if split:
        drawn = drawn * levels(stream_key, dims, split, -0.22, 0.18)
    return jnp.clip(strengthened(drawn, jax.random.fold_in(stream_key, 3), *heavy), -most, most).astype(held_as)


def setup_inputs(seed: int = 0, part: int = 0) -> dict:
    streams_of = jax.random.split(jax.random.key(seed), 8)
    part_splits = jax.random.split(jax.random.fold_in(streams_of[7], part), 8)
    tokens = gaussian(part_splits[0], (TOKENS, D), 1.0, 6.0, ((0, 4),))
    routes_keys = jax.random.split(jax.random.fold_in(part_splits[1], 1), TOKENS // TOK_DEV)
    routes_turns = jax.random.permutation(jax.random.fold_in(part_splits[1], 3), TOKENS // TOK_DEV)
    routes = jax.vmap(lambda own, number: routed_block(jax.random.fold_in(part_splits[1], 2), own, number, TOK_DEV, EXPERTS, TOP, CAP, 1))(routes_keys, routes_turns).reshape((TOKENS, TOP))
    route_weight = jnp.clip(0.2 + 0.8 * jax.random.uniform(part_splits[2], (TOKENS, TOP), jnp.float32) ** levels(part_splits[2], (TOKENS, TOP), ((0, 4),), -0.2, 0.2), 0.2, 1.0)
    norm_gain = jnp.clip(1.0 + 0.18 * jax.random.normal(streams_of[3], (D,), jnp.float32), 0.1, 1.9)
    gate_train = gaussian(streams_of[4], (EXPERTS, D, FF), D ** -0.5, 0.125, ((0, 4), (1, 64)), jnp.float32)
    up_train = gaussian(streams_of[5], (EXPERTS, D, FF), D ** -0.5, 0.125, ((0, 4), (1, 64)), jnp.float32)
    down_train = gaussian_with(streams_of[6], (EXPERTS, FF, D), FF ** -0.5, 0.21875, ((0, 4), (2, 64)), (1, 2, 64, 4.0), jnp.float32)
    return {"tokens": tokens, "routes": routes, "route_weight": route_weight, "norm_gain": norm_gain, "gate_train": gate_train, "up_train": up_train, "down_train": down_train}


def reference(tokens, routes, route_weight, norm_gain, gate_train, up_train, down_train):
    gain_column = norm_gain[None, :, None]
    gate_low = (gate_train * gain_column).astype(jnp.bfloat16)
    up_low = (up_train * gain_column).astype(jnp.bfloat16)
    down_low = down_train.astype(jnp.bfloat16)
    tok_float = tokens.astype(jnp.float32)
    normed = (tok_float * lax.rsqrt(lax.optimization_barrier(jnp.mean(tok_float * tok_float, axis=-1, keepdims=True)) + 1e-06)).astype(jnp.bfloat16)
    normed_wide = normed.astype(jnp.float32)

    def expert(triple):
        gate_one, up_one, down_one = triple
        gated = jnp.dot(normed_wide, gate_one.astype(jnp.float32), preferred_element_type=jnp.float32)
        lifted = jnp.dot(normed_wide, up_one.astype(jnp.float32), preferred_element_type=jnp.float32)
        hidden = (jax.nn.silu(gated) * lifted).astype(jnp.bfloat16)
        return jnp.dot(hidden.astype(jnp.float32), down_one.astype(jnp.float32), preferred_element_type=jnp.float32).astype(jnp.bfloat16)
    outputs = lax.map(expert, (gate_low, up_low, down_low))
    row_index = jnp.arange(tokens.shape[0], dtype=jnp.int32)
    first = outputs[routes[:, 0], row_index].astype(jnp.float32)
    second = outputs[routes[:, 1], row_index].astype(jnp.float32)
    mixed = route_weight[:, 0:1] * first + route_weight[:, 1:2] * second
    gate_serve = jnp.tile(gate_low, (1, 1, COPIES))
    up_serve = jnp.tile(up_low, (1, 1, COPIES))
    down_serve = jnp.tile(down_low, (1, COPIES, 1))
    return (gate_serve, up_serve, down_serve, mixed.astype(jnp.bfloat16))
```

```python
import functools

import jax
import jax.numpy as jnp
from jax import lax
from jax.experimental import pallas as pl
from jax.experimental.pallas import tpu as pltpu
from jax.sharding import Mesh
from jax.sharding import PartitionSpec as P

EXPERTS = 4
CAP = 128
FS = ("fs_0", "fs_1")
MESH = pl.DeviceIdType.MESH
LANES = 128


def exchange_kernel(
    groups,
    chips,
    gate,
    up,
    down,
    gate_out,
    up_out,
    down_out,
    rows_buf,
    tile_buf,
    quad_send,
    quad_recv,
    ring_send,
    unit_recv,
    group_send,
):
    g = lax.axis_index("grp")
    z = lax.axis_index("fs_0")
    c = lax.axis_index("fs_1")
    quads = chips // 2
    half_ring = chips // 2
    rows, hidden = gate.shape
    units = gate_out.shape[0]
    spread = groups // 2
    share = hidden // 4
    blocks = share // units
    own_count = quads // groups
    q = z // 2
    odd = lax.rem(z, 2)
    me = 2 * odd + c
    half = lax.rem(g + q // spread, 2)
    active = lax.rem(q, spread) == g // 2
    my_block = 2 * lax.rem(z, half_ring) + c
    my_half = my_block // (2 * blocks)
    my_source_core = lax.rem(my_block, 2 * blocks) // blocks
    parity = lax.rem(my_half + g, 2)
    own = jnp.logical_and(active, jnp.logical_and(half == my_half, c == my_source_core))
    inputs = (gate, up, down)
    outputs = (gate_out, up_out, down_out)

    def at(chip, core):
        return {"fs_0": chip, "fs_1": core}

    def own_quad(j):
        return spread * (2 * j + parity) + g // 2

    def sender_of(other):
        right = lax.rem(z - (2 * other + 1) + chips, chips) < half_ring
        return 2 * other + jnp.where(right, 1, 0)

    def target(i):
        chip = half * blocks + c * (blocks // 2) + i // 2
        right = lax.rem(chip - z + 2 * chips, half_ring)
        left = lax.rem(z - chip + 2 * chips, half_ring)
        chip = jnp.where(odd == 1, z + right, z - left + chips)
        return lax.rem(chip, chips), lax.rem(i, 2)

    def place(index):
        return pl.ds(pl.multiple_of(index * LANES, LANES), LANES)

    quad_mates = ((z + 1 - 2 * odd, c), (z, 1 - c), (z + 1 - 2 * odd, 1 - c))

    barrier = pltpu.get_barrier_semaphore()

    @pl.when(active)
    def _():
        for chip, core in quad_mates:
            pl.semaphore_signal(barrier, inc=1, device_id=at(chip, core), device_id_type=MESH)

    def greet(j, _):
        other = own_quad(j)
        chip = sender_of(other)

        @pl.when(jnp.logical_not(jnp.logical_and(own, other == q)))
        def _():
            pl.semaphore_signal(
                barrier, inc=1, device_id=at(chip, my_source_core), device_id_type=MESH
            )

        return 0

    lax.fori_loop(0, own_count, greet, 0)
    for step in range(1, groups):
        pl.semaphore_signal(
            barrier, inc=1, device_id={"grp": lax.rem(g + step, groups)}, device_id_type=MESH
        )
    expected = jnp.where(active, 3 + blocks - jnp.where(own, 1, 0), 0) + groups - 1
    pl.semaphore_wait(barrier, expected)

    def lanes_for(core):
        return pl.ds(pl.multiple_of((2 * half + core) * share, LANES), share)

    def rows_at(index):
        return pl.ds(pl.multiple_of(index * rows, rows), rows)

    def mate_copy(m, k):
        chip, core = quad_mates[k]
        return pltpu.make_async_remote_copy(
            src_ref=inputs[m].at[:, lanes_for(core)],
            dst_ref=rows_buf.at[m, rows_at(me), :],
            send_sem=quad_send.at[m, k],
            recv_sem=quad_recv.at[m, me],
            device_id=at(chip, core),
            device_id_type=MESH,
        )

    def own_copy(m):
        return pltpu.make_async_copy(
            inputs[m].at[:, lanes_for(c)], rows_buf.at[m, rows_at(me), :], quad_recv.at[m, me]
        )

    def ring_copy(m, i):
        chip, core = target(i)
        return pltpu.make_async_remote_copy(
            src_ref=tile_buf.at[m, pl.ds(pl.multiple_of(i * units, 16), units), :],
            dst_ref=outputs[m].at[:, place(q)],
            send_sem=ring_send.at[m, i],
            recv_sem=unit_recv.at[m, q],
            device_id=at(chip, core),
            device_id_type=MESH,
        )

    def group_copy(m, j, step):
        other = own_quad(j)
        return pltpu.make_async_remote_copy(
            src_ref=outputs[m].at[:, place(other)],
            dst_ref=outputs[m].at[:, place(other)],
            send_sem=group_send.at[m, j, step - 1],
            recv_sem=unit_recv.at[m, other],
            device_id={"grp": lax.rem(g + step, groups)},
            device_id_type=MESH,
        )

    def unit_arrival(m, index):
        return pltpu.make_async_remote_copy(
            src_ref=outputs[m].at[:, place(index)],
            dst_ref=outputs[m].at[:, place(index)],
            send_sem=group_send.at[m, 0, 0],
            recv_sem=unit_recv.at[m, index],
            device_id={"grp": lax.rem(g + 1, groups)},
            device_id_type=MESH,
        )

    def is_mine(i):
        chip, core = target(i)
        return jnp.logical_and(chip == z, core == c)

    @pl.when(active)
    def _():
        for m in range(3):
            own_copy(m).start()
            for k in range(3):
                mate_copy(m, k).start()
        for m in range(3):
            own_copy(m).wait()
            for k in range(3):
                chip_back, core_back = quad_mates[k]
                source = 2 * lax.rem(chip_back, 2) + core_back
                pltpu.make_async_remote_copy(
                    src_ref=inputs[m].at[:, lanes_for(c)],
                    dst_ref=rows_buf.at[m, rows_at(source), :],
                    send_sem=quad_send.at[m, k],
                    recv_sem=quad_recv.at[m, source],
                    device_id=at(chip_back, core_back),
                    device_id_type=MESH,
                ).wait_recv()
            tile_buf[m, :, :] = rows_buf[m, :, :].T

            def send(i, _):
                mine = is_mine(i)

                @pl.when(mine)
                def _():
                    outputs[m][:, place(q)] = tile_buf[
                        m, pl.ds(pl.multiple_of(i * units, 16), units), :
                    ]

                @pl.when(jnp.logical_not(mine))
                def _():
                    ring_copy(m, i).start()

                return 0

            lax.fori_loop(0, blocks, send, 0)

    for m in range(3):

        def forward(j, _):
            other = own_quad(j)

            @pl.when(jnp.logical_not(jnp.logical_and(own, other == q)))
            def _():
                unit_arrival(m, other).wait_recv()

            for step in range(1, groups):
                group_copy(m, j, step).start()
            return 0

        lax.fori_loop(0, own_count, forward, 0)

    for m in range(3):

        def arrive(index, _):
            here = jnp.logical_and(
                lax.rem(index, spread) == g // 2, lax.rem(index // spread, 2) == parity
            )

            @pl.when(jnp.logical_not(here))
            def _():
                unit_arrival(m, index).wait_recv()

            return 0

        lax.fori_loop(0, quads, arrive, 0)

    for m in range(3):

        @pl.when(active)
        def _():
            for k in range(3):
                mate_copy(m, k).wait_send()

            def sent(i, _):
                @pl.when(jnp.logical_not(is_mine(i)))
                def _():
                    ring_copy(m, i).wait_send()

                return 0

            lax.fori_loop(0, blocks, sent, 0)

        def passed(j, _):
            for step in range(1, groups):
                group_copy(m, j, step).wait_send()
            return 0

        lax.fori_loop(0, own_count, passed, 0)


def exchange(groups, chips, gate_low, up_low, down_low):
    rows, hidden = gate_low.shape
    units = hidden // chips
    width = rows * 2 * chips
    quads = chips // 2
    share = hidden // 4
    served = jax.ShapeDtypeStruct((units, width), jnp.bfloat16)
    return pl.pallas_call(
        functools.partial(exchange_kernel, groups, chips),
        out_shape=(served, served, served),
        in_specs=[pl.BlockSpec(memory_space=pl.ANY)] * 3,
        out_specs=[pl.BlockSpec(memory_space=pltpu.VMEM)] * 3,
        scratch_shapes=[
            pltpu.VMEM((3, 4 * rows, share), jnp.bfloat16),
            pltpu.VMEM((3, share, 4 * rows), jnp.bfloat16),
            pltpu.SemaphoreType.DMA((3, 3)),
            pltpu.SemaphoreType.DMA((3, 4)),
            pltpu.SemaphoreType.DMA((3, share // units)),
            pltpu.SemaphoreType.DMA((3, quads)),
            pltpu.SemaphoreType.DMA((3, quads // groups, groups - 1)),
        ],
        compiler_params=pltpu.CompilerParams(collective_id=0, has_side_effects=True),
        name="exchange",
    )(gate_low, up_low, down_low)


def shards(tokens, routes, route_weight, norm_gain, gate_train, up_train, down_train):
    fs_count = lax.axis_size(FS)
    chips = lax.axis_size("fs_0")
    groups = lax.axis_size("grp")
    pieces = chips
    copies = fs_count // pieces
    gain_column = norm_gain[:, None]
    gate_low = (gate_train[0] * gain_column).astype(jnp.bfloat16)
    up_low = (up_train[0] * gain_column).astype(jnp.bfloat16)
    down_low = down_train[0].T.astype(jnp.bfloat16)
    gate_new, up_new, down_new = exchange(groups, chips, gate_low, up_low, down_low)
    tok_float = tokens.astype(jnp.float32)
    normed = (
        tok_float * lax.rsqrt(jnp.mean(tok_float * tok_float, axis=-1, keepdims=True) + 1e-06)
    ).astype(jnp.bfloat16)
    chosen = routes.reshape(-1)
    chosen_hot = (chosen[:, None] == jnp.arange(EXPERTS, dtype=jnp.int32)[None, :]).astype(
        jnp.int32
    )
    before = jnp.cumsum(chosen_hot, axis=0) - chosen_hot
    slot_rank = jnp.sum(before * chosen_hot, axis=1)
    slot_index = (chosen * CAP + slot_rank).reshape(routes.shape)
    slot_range = jnp.arange(EXPERTS * CAP, dtype=jnp.int32)
    select_rows = jnp.any(slot_range[:, None, None] == slot_index[None, :, :], axis=-1).astype(
        jnp.bfloat16
    )
    outgoing = jnp.dot(select_rows, normed, preferred_element_type=jnp.float32).astype(jnp.bfloat16)
    outgoing = outgoing.reshape(EXPERTS, CAP, normed.shape[1])
    arrived = lax.all_to_all(outgoing, "tp", split_axis=0, concat_axis=0, tiled=True).reshape(
        EXPERTS * CAP, normed.shape[1]
    )
    slot_count = EXPERTS * CAP // copies
    copy_index = lax.axis_index(FS) // pieces
    my_rows = lax.dynamic_slice_in_dim(arrived, copy_index * slot_count, slot_count, 0)
    dims = (((1,), (1,)), ((), ()))
    gated = lax.dot_general(gate_new, my_rows, dims, preferred_element_type=jnp.float32)
    lifted = lax.dot_general(up_new, my_rows, dims, preferred_element_type=jnp.float32)
    hidden = (jax.nn.silu(gated) * lifted).astype(jnp.bfloat16)
    every = lax.all_gather(hidden, FS)
    every = every.reshape(copies, pieces * hidden.shape[0], slot_count)
    expert_out = jnp.einsum(
        "cu,kus->kcs", down_low, every, preferred_element_type=jnp.float32
    ).astype(jnp.bfloat16)
    columns = expert_out.shape[1]
    back = jnp.moveaxis(expert_out.reshape(copies, columns, EXPERTS // copies, CAP), 2, 1)
    returned = lax.all_to_all(
        back.reshape(EXPERTS, columns, CAP), "tp", split_axis=0, concat_axis=0, tiled=True
    )
    blend_weight = jnp.sum(
        jnp.where(
            slot_range[None, None, :] == slot_index[:, :, None], route_weight[:, :, None], 0.0
        ),
        axis=1,
    ).reshape(-1, EXPERTS, CAP)
    mixed = jnp.einsum(
        "tes,ecs->tc",
        blend_weight,
        returned.astype(jnp.float32),
        preferred_element_type=jnp.float32,
    )
    return (gate_new.T[None], up_new.T[None], down_new[None], mixed.astype(jnp.bfloat16))


def solution(mesh):
    cores = 2
    split = Mesh(
        mesh.devices.reshape(
            mesh.shape["grp"], mesh.shape["fs"] // cores, cores, mesh.shape["tp"]
        ),
        ("grp", "fs_0", "fs_1", "tp"),
    )
    placed = (
        P(("grp", "tp"), None),
        P(("grp", "tp"), None),
        P(("grp", "tp"), None),
        P(FS),
        P("tp", FS, None),
        P("tp", FS, None),
        P("tp", None, FS),
    )
    return jax.shard_map(
        shards,
        mesh=split,
        in_specs=placed,
        out_specs=(
            P(("grp", "tp"), None, FS),
            P(("grp", "tp"), None, FS),
            P(("grp", "tp"), FS, None),
            P(("grp", "tp"), FS),
        ),
        check_vma=False,
    )
```

```python
import functools

import jax
import jax.numpy as jnp
from jax import lax
from jax.experimental import pallas as pl
from jax.experimental.pallas import tpu as pltpu
from jax.sharding import Mesh
from jax.sharding import PartitionSpec as P

CAP = 128
LANES = 128
FS = ("fs_0", "fs_1")
MESH = pl.DeviceIdType.MESH
NT = (((1,), (1,)), ((), ()))


def layer_kernel(
    groups,
    chips,
    experts,
    tokens,
    routes,
    route_weight,
    gain,
    gate,
    up,
    down,
    gate_out,
    up_out,
    down_out,
    mixed_out,
    low,
    rows_buf,
    tile_buf,
    select,
    outgoing,
    arrived,
    turned,
    picked,
    split_down,
    my_down,
    hidden_all,
    partial,
    partial_in,
    column_out,
    returned,
    quad_send,
    quad_recv,
    ring_send,
    unit_recv,
    group_send,
    token_send,
    token_recv,
    core_send,
    core_recv,
    hop_send,
    hop_recv,
    back_send,
    back_recv,
):
    g = lax.axis_index("grp")
    z = lax.axis_index("fs_0")
    c = lax.axis_index("fs_1")
    t = lax.axis_index("tp")
    quads = chips // 2
    half_ring = chips // 2
    rows, hidden = gate.shape
    units = gate_out.shape[0]
    spread = groups // 2
    share = hidden // 4
    blocks = share // units
    own_count = quads // groups
    slots = experts * CAP
    q = z // 2
    odd = lax.rem(z, 2)
    me = 2 * odd + c
    half = lax.rem(g + q // spread, 2)
    active = lax.rem(q, spread) == g // 2
    pair = lax.rem(z, half_ring)
    my_block = 2 * pair + c
    my_half = my_block // (2 * blocks)
    my_source_core = lax.rem(my_block, 2 * blocks) // blocks
    parity = lax.rem(my_half + g, 2)
    own = jnp.logical_and(active, jnp.logical_and(half == my_half, c == my_source_core))
    outputs = (gate_out, up_out, down_out)
    reach = half_ring // 2

    def at(chip, core):
        return {"fs_0": chip, "fs_1": core}

    def own_quad(j):
        return spread * (2 * j + parity) + g // 2

    def sender_of(other):
        right = lax.rem(z - (2 * other + 1) + chips, chips) < half_ring
        return 2 * other + jnp.where(right, 1, 0)

    def target(i):
        chip = half * blocks + c * (blocks // 2) + i // 2
        right = lax.rem(chip - z + 2 * chips, half_ring)
        left = lax.rem(z - chip + 2 * chips, half_ring)
        chip = jnp.where(odd == 1, z + right, z - left + chips)
        return lax.rem(chip, chips), lax.rem(i, 2)

    def place(index):
        return pl.ds(pl.multiple_of(index * LANES, LANES), LANES)

    def block_rows(index):
        return pl.ds(pl.multiple_of(index * units, 16), units)

    def rows_at(index):
        return pl.ds(pl.multiple_of(index * rows, rows), rows)

    quad_mates = ((z + 1 - 2 * odd, c), (z, 1 - c), (z + 1 - 2 * odd, 1 - c))
    next_chip = lax.rem(z + 1, chips)
    last_chip = lax.rem(z + chips - 1, chips)

    barrier = pltpu.get_barrier_semaphore()

    def greet_device(where):
        pl.semaphore_signal(barrier, inc=1, device_id=where, device_id_type=MESH)

    def greet(j, _):
        other = own_quad(j)
        chip = sender_of(other)

        @pl.when(jnp.logical_not(jnp.logical_and(own, other == q)))
        def _():
            greet_device(at(chip, my_source_core))

        return 0

    lax.fori_loop(0, own_count, greet, 0)
    for chip, core in quad_mates:
        greet_device(at(chip, core))
    for step in range(1, groups):
        greet_device({"grp": lax.rem(g + step, groups)})
    for step in range(1, experts):
        greet_device({"tp": lax.rem(t + step, experts)})
    greet_device(at(next_chip, c))
    greet_device(at(last_chip, c))

    eye = lax.broadcasted_iota(jnp.int32, (rows, rows), 0) == lax.broadcasted_iota(
        jnp.int32, (rows, rows), 1
    )
    gain_column = jnp.sum(jnp.where(eye, gain[...], 0.0), axis=1, keepdims=True)
    low[0, :, :] = (gate[...] * gain_column).astype(jnp.bfloat16)
    low[1, :, :] = (up[...] * gain_column).astype(jnp.bfloat16)
    low[2, :, :] = down[...].astype(jnp.bfloat16)

    token_count, width = tokens.shape
    first = routes[0:1, :]
    second = routes[1:2, :]
    expert_row = lax.broadcasted_iota(jnp.int32, (8, token_count), 0)
    named = jnp.logical_or(first == expert_row, second == expert_row)
    before = (
        lax.broadcasted_iota(jnp.int32, (token_count, token_count), 0)
        < lax.broadcasted_iota(jnp.int32, (token_count, token_count), 1)
    )
    rank = jnp.dot(
        jnp.where(named, 1.0, 0.0).astype(jnp.bfloat16),
        jnp.where(before, 1.0, 0.0).astype(jnp.bfloat16),
        preferred_element_type=jnp.float32,
    )
    slot = lax.broadcasted_iota(jnp.int32, (CAP, token_count), 0).astype(jnp.float32)
    tok_float = tokens[...].astype(jnp.float32)
    normed = (
        tok_float * lax.rsqrt(jnp.mean(tok_float * tok_float, axis=-1, keepdims=True) + 1e-06)
    ).astype(jnp.bfloat16)
    for e in range(experts):
        chosen = jnp.logical_or(first == e, second == e)
        hot = jnp.logical_and(slot == rank[e : e + 1, :], chosen)
        select[e, :, :] = jnp.where(hot, 1.0, 0.0).astype(jnp.bfloat16)
        outgoing[e, :, :] = jnp.dot(
            select[e, :, :], normed, preferred_element_type=jnp.float32
        ).astype(jnp.bfloat16)

    expected = jnp.where(active, blocks - jnp.where(own, 1, 0), 0)
    pl.semaphore_wait(barrier, expected + groups - 1 + 3 + experts - 1 + 2)

    def lanes_for(core):
        return pl.ds(pl.multiple_of((2 * half + core) * share, LANES), share)

    def mate_copy(m, k):
        chip, core = quad_mates[k]
        return pltpu.make_async_remote_copy(
            src_ref=low.at[m, :, lanes_for(core)],
            dst_ref=rows_buf.at[m, rows_at(me), :],
            send_sem=quad_send.at[m, k],
            recv_sem=quad_recv.at[m, me],
            device_id=at(chip, core),
            device_id_type=MESH,
        )

    def ring_copy(m, i):
        chip, core = target(i)
        return pltpu.make_async_remote_copy(
            src_ref=tile_buf.at[m, block_rows(i), :],
            dst_ref=outputs[m].at[:, place(q)],
            send_sem=ring_send.at[m, i],
            recv_sem=unit_recv.at[m, q],
            device_id=at(chip, core),
            device_id_type=MESH,
        )

    def group_copy(m, j, step):
        other = own_quad(j)
        return pltpu.make_async_remote_copy(
            src_ref=outputs[m].at[:, place(other)],
            dst_ref=outputs[m].at[:, place(other)],
            send_sem=group_send.at[m, j, step - 1],
            recv_sem=unit_recv.at[m, other],
            device_id={"grp": lax.rem(g + step, groups)},
            device_id_type=MESH,
        )

    def unit_arrival(m, index):
        return pltpu.make_async_remote_copy(
            src_ref=outputs[m].at[:, place(index)],
            dst_ref=outputs[m].at[:, place(index)],
            send_sem=group_send.at[m, 0, 0],
            recv_sem=unit_recv.at[m, index],
            device_id={"grp": lax.rem(g + 1, groups)},
            device_id_type=MESH,
        )

    def is_mine(i):
        chip, core = target(i)
        return jnp.logical_and(chip == z, core == c)

    def token_copy(step):
        other = lax.rem(t + step, experts)
        return pltpu.make_async_remote_copy(
            src_ref=outgoing.at[other],
            dst_ref=arrived.at[t],
            send_sem=token_send.at[step - 1],
            recv_sem=token_recv.at[t],
            device_id={"tp": other},
            device_id_type=MESH,
        )

    def token_arrival(step):
        other = lax.rem(t + step, experts)
        return pltpu.make_async_remote_copy(
            src_ref=outgoing.at[other],
            dst_ref=arrived.at[other],
            send_sem=token_send.at[step - 1],
            recv_sem=token_recv.at[other],
            device_id={"tp": other},
            device_id_type=MESH,
        )

    @pl.when(active)
    def _():
        for m in range(3):
            for k in range(3):
                mate_copy(m, k).start()
        for step in range(1, experts):
            token_copy(step).start()
        for m in range(3):
            rows_buf[m, rows_at(me), :] = low[m, :, lanes_for(c)]
            for k in range(3):
                chip_back, core_back = quad_mates[k]
                source = 2 * lax.rem(chip_back, 2) + core_back
                pltpu.make_async_remote_copy(
                    src_ref=low.at[m, :, lanes_for(c)],
                    dst_ref=rows_buf.at[m, rows_at(source), :],
                    send_sem=quad_send.at[m, k],
                    recv_sem=quad_recv.at[m, source],
                    device_id=at(chip_back, core_back),
                    device_id_type=MESH,
                ).wait_recv()
            tile_buf[m, :, :] = rows_buf[m, :, :].T

            def send(i, _):
                mine = is_mine(i)

                @pl.when(mine)
                def _():
                    outputs[m][:, place(q)] = tile_buf[m, block_rows(i), :]

                @pl.when(jnp.logical_not(mine))
                def _():
                    ring_copy(m, i).start()

                return 0

            lax.fori_loop(0, blocks, send, 0)

    @pl.when(jnp.logical_not(active))
    def _():
        for step in range(1, experts):
            token_copy(step).start()

    arrived[t] = outgoing[t]

    chunk = 4 * LANES

    def turn(k, _):
        lanes = pl.ds(pl.multiple_of(k * chunk, chunk), chunk)
        tall = jnp.concatenate(
            [down[:, lanes], jnp.zeros((LANES - rows, chunk), jnp.float32)], axis=0
        )
        turned[lanes, :] = tall.T.astype(jnp.bfloat16)
        return 0

    lax.fori_loop(0, hidden // chunk, turn, 0)

    def pick(k, _):
        for p in range(2):
            picked[p, block_rows(k), :] = turned[block_rows(2 * k + p), :]
        return 0

    lax.fori_loop(0, half_ring, pick, 0)
    piece = 2 * LANES

    def lay(k, _):
        span = pl.ds(pl.multiple_of(k * piece, piece), piece)
        for p in range(2):
            split_down[p, :, span] = picked[p, span, :].T[:rows, :]
        return 0

    lax.fori_loop(0, hidden // 2 // piece, lay, 0)
    my_down[rows_at(c), :] = split_down[c]
    columns_copy = pltpu.make_async_remote_copy(
        src_ref=split_down.at[1 - c],
        dst_ref=my_down.at[rows_at(c), :],
        send_sem=core_send.at[0],
        recv_sem=core_recv.at[0],
        device_id=at(z, 1 - c),
        device_id_type=MESH,
    )
    columns_copy.start()

    def forward(m, j):
        other = own_quad(j)

        @pl.when(jnp.logical_not(jnp.logical_and(own, other == q)))
        def _():
            unit_arrival(m, other).wait_recv()

        for step in range(1, groups):
            group_copy(m, j, step).start()

    def arrive(m):
        def body(index, _):
            here = jnp.logical_and(
                lax.rem(index, spread) == g // 2, lax.rem(index // spread, 2) == parity
            )

            @pl.when(jnp.logical_not(here))
            def _():
                unit_arrival(m, index).wait_recv()

            return 0

        lax.fori_loop(0, quads, body, 0)

    for m in range(2):

        def body(j, _):
            forward(m, j)
            return 0

        lax.fori_loop(0, own_count, body, 0)
    for m in range(2):
        arrive(m)
    for step in range(1, experts):
        token_arrival(step).wait_recv()

    wide = slots // 2

    def hide(k, _):
        own_tokens = arrived[pl.ds(k * (experts // 2), experts // 2)].reshape(wide, width)
        gated = lax.dot_general(gate_out[...], own_tokens, NT, preferred_element_type=jnp.float32)
        lifted = lax.dot_general(up_out[...], own_tokens, NT, preferred_element_type=jnp.float32)
        hidden_all[k, block_rows(pair), :] = (
            gated * (1.0 / (1.0 + jnp.exp(-gated))) * lifted
        ).astype(jnp.bfloat16)
        return 0

    lax.fori_loop(0, 2, hide, 0)

    def hop_copy(way, k, step):
        chip = lax.rem(z + chips - step if way == 0 else z + step, half_ring)
        return pltpu.make_async_remote_copy(
            src_ref=hidden_all.at[k, block_rows(chip), :],
            dst_ref=hidden_all.at[k, block_rows(chip), :],
            send_sem=hop_send.at[way, k, step],
            recv_sem=hop_recv.at[way, k, step],
            device_id=at(next_chip if way == 0 else last_chip, c),
            device_id_type=MESH,
        )

    def hop_arrival(way, k, step):
        chip = lax.rem(z + chips - step - 1 if way == 0 else z + step + 1, half_ring)
        return pltpu.make_async_remote_copy(
            src_ref=hidden_all.at[k, block_rows(chip), :],
            dst_ref=hidden_all.at[k, block_rows(chip), :],
            send_sem=hop_send.at[way, k, step],
            recv_sem=hop_recv.at[way, k, step],
            device_id=at(last_chip if way == 0 else next_chip, c),
            device_id_type=MESH,
        )

    for k in range(2):
        for way in range(2):
            hop_copy(way, k, 0).start()

    def hop(step, _):
        @pl.when(step < own_count)
        def _():
            forward(2, step)

        for k in range(2):
            for way in range(2):
                hop_arrival(way, k, step).wait_recv()

                @pl.when(jnp.logical_or(step < reach - 2, k == way))
                def _():
                    hop_copy(way, k, step + 1).start()

        return 0

    lax.fori_loop(0, reach - 1, hop, 0)
    for j in range(reach - 1, own_count):
        forward(2, j)
    for way in range(2):
        hop_arrival(way, way, reach - 1).wait_recv()
    columns_copy.wait()

    for k in range(2):
        partial[k, :, :] = jnp.dot(
            my_down[...], hidden_all[k, :, :], preferred_element_type=jnp.float32
        )

    partial_copy = pltpu.make_async_remote_copy(
        src_ref=partial.at[:, rows_at(1 - c), :],
        dst_ref=partial_in,
        send_sem=core_send.at[1],
        recv_sem=core_recv.at[1],
        device_id=at(z, 1 - c),
        device_id_type=MESH,
    )
    partial_copy.start()
    partial_copy.wait_recv()
    for e in range(experts):
        k, lane = e // (experts // 2), (e % (experts // 2)) * CAP
        lanes = pl.ds(lane, CAP)
        column_out[e, :, :] = (
            partial[k, rows_at(c), lanes] + partial_in[k, :, lanes]
        ).astype(jnp.bfloat16)

    def back_copy(step):
        other = lax.rem(t + step, experts)
        return pltpu.make_async_remote_copy(
            src_ref=column_out.at[other],
            dst_ref=returned.at[t],
            send_sem=back_send.at[step - 1],
            recv_sem=back_recv.at[t],
            device_id={"tp": other},
            device_id_type=MESH,
        )

    def back_arrival(step):
        other = lax.rem(t + step, experts)
        return pltpu.make_async_remote_copy(
            src_ref=column_out.at[other],
            dst_ref=returned.at[other],
            send_sem=back_send.at[step - 1],
            recv_sem=back_recv.at[other],
            device_id={"tp": other},
            device_id_type=MESH,
        )

    for step in range(1, experts):
        back_copy(step).start()
    returned[t] = column_out[t]
    for step in range(1, experts):
        back_arrival(step).wait_recv()
    total = jnp.zeros((rows, token_count), jnp.float32)
    for e in range(experts):
        weight = jnp.where(first == e, route_weight[0:1, :], 0.0) + jnp.where(
            second == e, route_weight[1:2, :], 0.0
        )
        total = total + weight * jnp.dot(
            returned[e, :, :], select[e, :, :], preferred_element_type=jnp.float32
        )
    mixed_out[...] = total.astype(jnp.bfloat16)

    arrive(2)
    for m in range(3):

        @pl.when(active)
        def _():
            for k in range(3):
                mate_copy(m, k).wait_send()

            def sent(i, _):
                @pl.when(jnp.logical_not(is_mine(i)))
                def _():
                    ring_copy(m, i).wait_send()

                return 0

            lax.fori_loop(0, blocks, sent, 0)

        def passed(j, _):
            for step in range(1, groups):
                group_copy(m, j, step).wait_send()
            return 0

        lax.fori_loop(0, own_count, passed, 0)

    def hopped(step, _):
        for k in range(2):
            for way in range(2):

                @pl.when(jnp.logical_or(step < reach - 1, k == way))
                def _():
                    hop_copy(way, k, step).wait_send()

        return 0

    lax.fori_loop(0, reach, hopped, 0)
    partial_copy.wait_send()
    for step in range(1, experts):
        token_copy(step).wait_send()
        back_copy(step).wait_send()


def layer(groups, chips, experts, *operands):
    tokens, _, _, _, gate, _, _ = operands
    rows, hidden = gate.shape
    units = hidden // chips
    width = rows * 2 * chips
    quads = chips // 2
    share = hidden // 4
    reach = chips // 4
    wide = experts * CAP // 2
    served = jax.ShapeDtypeStruct((units, width), jnp.bfloat16)
    dma = pltpu.SemaphoreType.DMA
    return pl.pallas_call(
        functools.partial(layer_kernel, groups, chips, experts),
        out_shape=(
            served,
            served,
            served,
            jax.ShapeDtypeStruct((rows, tokens.shape[0]), jnp.bfloat16),
        ),
        in_specs=[pl.BlockSpec(memory_space=pltpu.VMEM)] * 7,
        out_specs=[pl.BlockSpec(memory_space=pltpu.VMEM)] * 4,
        scratch_shapes=[
            pltpu.VMEM((3, rows, hidden), jnp.bfloat16),
            pltpu.VMEM((3, 4 * rows, share), jnp.bfloat16),
            pltpu.VMEM((3, share, 4 * rows), jnp.bfloat16),
            pltpu.VMEM((experts, CAP, tokens.shape[0]), jnp.bfloat16),
            pltpu.VMEM((experts, CAP, width), jnp.bfloat16),
            pltpu.VMEM((experts, CAP, width), jnp.bfloat16),
            pltpu.VMEM((hidden, LANES), jnp.bfloat16),
            pltpu.VMEM((2, hidden // 2, LANES), jnp.bfloat16),
            pltpu.VMEM((2, rows, hidden // 2), jnp.bfloat16),
            pltpu.VMEM((2 * rows, hidden // 2), jnp.bfloat16),
            pltpu.VMEM((2, hidden // 2, wide), jnp.bfloat16),
            pltpu.VMEM((2, 2 * rows, wide), jnp.float32),
            pltpu.VMEM((2, rows, wide), jnp.float32),
            pltpu.VMEM((experts, rows, CAP), jnp.bfloat16),
            pltpu.VMEM((experts, rows, CAP), jnp.bfloat16),
            dma((3, 3)),
            dma((3, 4)),
            dma((3, share // units)),
            dma((3, quads)),
            dma((3, quads // groups, groups - 1)),
            dma((experts - 1,)),
            dma((experts,)),
            dma((2,)),
            dma((2,)),
            dma((2, 2, reach)),
            dma((2, 2, reach)),
            dma((experts - 1,)),
            dma((experts,)),
        ],
        compiler_params=pltpu.CompilerParams(
            collective_id=0, has_side_effects=True, vmem_limit_bytes=48 * 1024 * 1024
        ),
        name="layer",
    )(*operands)


def shards(tokens, routes, route_weight, norm_gain, gate_train, up_train, down_train):
    gate_new, up_new, down_new, mixed = layer(
        lax.axis_size("grp"),
        lax.axis_size("fs_0"),
        lax.axis_size("tp"),
        tokens,
        routes.T,
        route_weight.T,
        norm_gain[None, :],
        gate_train[0],
        up_train[0],
        down_train[0].T,
    )
    return (gate_new.T[None], up_new.T[None], down_new[None], mixed.T)


def solution(mesh):
    cores = 2
    split = Mesh(
        mesh.devices.reshape(
            mesh.shape["grp"], mesh.shape["fs"] // cores, cores, mesh.shape["tp"]
        ),
        ("grp", "fs_0", "fs_1", "tp"),
    )
    placed = (
        P(("grp", "tp"), None),
        P(("grp", "tp"), None),
        P(("grp", "tp"), None),
        P(FS),
        P("tp", FS, None),
        P("tp", FS, None),
        P("tp", None, FS),
    )
    return jax.shard_map(
        shards,
        mesh=split,
        in_specs=placed,
        out_specs=(
            P(("grp", "tp"), None, FS),
            P(("grp", "tp"), None, FS),
            P(("grp", "tp"), FS, None),
            P(("grp", "tp"), FS),
        ),
        check_vma=False,
    )
```

```python
import functools

import jax
import jax.numpy as jnp
from jax import lax
from jax.experimental import pallas as pl
from jax.experimental.pallas import tpu as pltpu
from jax.sharding import Mesh
from jax.sharding import PartitionSpec as P

CAP = 128
LANES = 128
FS = ("fs_0", "fs_1")
MESH = pl.DeviceIdType.MESH
SUB = 2
NT = (((1,), (1,)), ((), ()))


def layer_kernel(
    groups,
    chips,
    experts,
    routes,
    route_weight,
    gain,
    tokens_far,
    gate_far,
    up_far,
    down_far,
    gate_out,
    up_out,
    down_out,
    mixed_out,
    tokens,
    full,
    low,
    rows_buf,
    tile_buf,
    select,
    outgoing,
    arrived,
    turned,
    picked,
    split_down,
    my_down,
    hidden_all,
    partial,
    partial_in,
    column_out,
    returned,
    quad_send,
    quad_recv,
    ring_send,
    unit_recv,
    group_send,
    token_send,
    token_recv,
    core_send,
    core_recv,
    hop_send,
    hop_recv,
    back_send,
    back_recv,
    read_sem,
):
    g = lax.axis_index("grp")
    z = lax.axis_index("fs_0")
    c = lax.axis_index("fs_1")
    t = lax.axis_index("tp")
    quads = chips // 2
    half_ring = chips // 2
    rows, hidden = gate_far.shape
    units = gate_out.shape[0]
    spread = groups // 2
    share = hidden // 4
    blocks = share // units
    own_count = quads // groups
    slots = experts * CAP
    q = z // 2
    odd = lax.rem(z, 2)
    me = 2 * odd + c
    half = lax.rem(g + q // spread, 2)
    active = lax.rem(q, spread) == g // 2
    pair = lax.rem(z, half_ring)
    my_block = 2 * pair + c
    my_half = my_block // (2 * blocks)
    my_source_core = lax.rem(my_block, 2 * blocks) // blocks
    parity = lax.rem(my_half + g, 2)
    own = jnp.logical_and(active, jnp.logical_and(half == my_half, c == my_source_core))
    outputs = (gate_out, up_out, down_out)
    reach = half_ring // 2

    def at(chip, core):
        return {"fs_0": chip, "fs_1": core}

    def own_quad(j):
        return spread * (2 * j + parity) + g // 2

    stride = blocks // own_count

    def turn_of(other):
        return lax.rem(other // spread // 2, own_count) * stride

    def expected_quad(n):
        place_in_list = lax.rem(my_block, blocks) // stride
        return own_quad(lax.rem(place_in_list - n + own_count, own_count))

    def sender_of(other):
        right = lax.rem(z - (2 * other + 1) + chips, chips) < half_ring
        return 2 * other + jnp.where(right, 1, 0)

    def target(i):
        chip = half * blocks + c * (blocks // 2) + i // 2
        right = lax.rem(chip - z + 2 * chips, half_ring)
        left = lax.rem(z - chip + 2 * chips, half_ring)
        chip = jnp.where(odd == 1, z + right, z - left + chips)
        return lax.rem(chip, chips), lax.rem(i, 2)

    def place(index):
        return pl.ds(pl.multiple_of(index * LANES, LANES), LANES)

    def block_rows(index):
        return pl.ds(pl.multiple_of(index * units, 16), units)

    def rows_at(index):
        return pl.ds(pl.multiple_of(index * rows, rows), rows)

    quad_mates = ((z + 1 - 2 * odd, c), (z, 1 - c), (z + 1 - 2 * odd, 1 - c))
    next_chip = lax.rem(z + 1, chips)
    last_chip = lax.rem(z + chips - 1, chips)

    reads = [
        pltpu.make_async_copy(far, full.at[m], read_sem.at[m])
        for m, far in enumerate((gate_far, up_far, down_far))
    ]
    reads.append(pltpu.make_async_copy(tokens_far, tokens, read_sem.at[3]))
    for read in reads:
        read.start()

    barrier = pltpu.get_barrier_semaphore()

    def greet_device(where):
        pl.semaphore_signal(barrier, inc=1, device_id=where, device_id_type=MESH)

    def greet(j, _):
        other = own_quad(j)
        chip = sender_of(other)

        @pl.when(jnp.logical_not(jnp.logical_and(own, other == q)))
        def _():
            greet_device(at(chip, my_source_core))

        return 0

    lax.fori_loop(0, own_count, greet, 0)
    for chip, core in quad_mates:
        greet_device(at(chip, core))
    for step in range(1, groups):
        greet_device({"grp": lax.rem(g + step, groups)})
    for step in range(1, experts):
        greet_device({"tp": lax.rem(t + step, experts)})
    greet_device(at(next_chip, c))
    greet_device(at(last_chip, c))

    eye = lax.broadcasted_iota(jnp.int32, (rows, rows), 0) == lax.broadcasted_iota(
        jnp.int32, (rows, rows), 1
    )
    gain_column = jnp.sum(jnp.where(eye, gain[...], 0.0), axis=1, keepdims=True)
    for m in range(2):
        reads[m].wait()
        low[m, :, :] = (full[m] * gain_column).astype(jnp.bfloat16)
    reads[2].wait()
    low[2, :, :] = full[2].astype(jnp.bfloat16)

    expected = jnp.where(active, blocks - jnp.where(own, 1, 0), 0)
    pl.semaphore_wait(barrier, expected + groups - 1 + 3 + experts - 1 + 2)

    def lanes_for(core):
        return pl.ds(pl.multiple_of((2 * half + core) * share, LANES), share)

    def mate_copy(m, k):
        chip, core = quad_mates[k]
        return pltpu.make_async_remote_copy(
            src_ref=low.at[m, :, lanes_for(core)],
            dst_ref=rows_buf.at[m, rows_at(me), :],
            send_sem=quad_send.at[m, k],
            recv_sem=quad_recv.at[m, me],
            device_id=at(chip, core),
            device_id_type=MESH,
        )

    def ring_copy(m, i):
        chip, core = target(i)
        return pltpu.make_async_remote_copy(
            src_ref=tile_buf.at[m, block_rows(i), :],
            dst_ref=outputs[m].at[:, place(q)],
            send_sem=ring_send.at[m, i],
            recv_sem=unit_recv.at[m, q],
            device_id=at(chip, core),
            device_id_type=MESH,
        )

    def group_copy(m, j, step):
        other = expected_quad(j)
        return pltpu.make_async_remote_copy(
            src_ref=outputs[m].at[:, place(other)],
            dst_ref=outputs[m].at[:, place(other)],
            send_sem=group_send.at[m, j, step - 1],
            recv_sem=unit_recv.at[m, other],
            device_id={"grp": lax.rem(g + step, groups)},
            device_id_type=MESH,
        )

    def unit_arrival(m, index):
        return pltpu.make_async_remote_copy(
            src_ref=outputs[m].at[:, place(index)],
            dst_ref=outputs[m].at[:, place(index)],
            send_sem=group_send.at[m, 0, 0],
            recv_sem=unit_recv.at[m, index],
            device_id={"grp": lax.rem(g + 1, groups)},
            device_id_type=MESH,
        )

    def is_mine(i):
        chip, core = target(i)
        return jnp.logical_and(chip == z, core == c)

    def token_copy(step):
        other = lax.rem(t + step, experts)
        return pltpu.make_async_remote_copy(
            src_ref=outgoing.at[other],
            dst_ref=arrived.at[t],
            send_sem=token_send.at[step - 1],
            recv_sem=token_recv.at[t],
            device_id={"tp": other},
            device_id_type=MESH,
        )

    def token_arrival(step):
        other = lax.rem(t + step, experts)
        return pltpu.make_async_remote_copy(
            src_ref=outgoing.at[other],
            dst_ref=arrived.at[other],
            send_sem=token_send.at[step - 1],
            recv_sem=token_recv.at[other],
            device_id={"tp": other},
            device_id_type=MESH,
        )

    @pl.when(active)
    def _():
        for m in range(3):
            for k in range(3):
                mate_copy(m, k).start()

    token_count, width = tokens.shape
    first = routes[0:1, :]
    second = routes[1:2, :]
    expert_row = lax.broadcasted_iota(jnp.int32, (8, token_count), 0)
    named = jnp.logical_or(first == expert_row, second == expert_row)
    before = (
        lax.broadcasted_iota(jnp.int32, (token_count, token_count), 0)
        < lax.broadcasted_iota(jnp.int32, (token_count, token_count), 1)
    )
    rank = jnp.dot(
        jnp.where(named, 1.0, 0.0).astype(jnp.bfloat16),
        jnp.where(before, 1.0, 0.0).astype(jnp.bfloat16),
        preferred_element_type=jnp.float32,
    )
    slot = lax.broadcasted_iota(jnp.int32, (CAP, token_count), 0).astype(jnp.float32)
    reads[3].wait()
    tok_float = tokens[...].astype(jnp.float32)
    normed = (
        tok_float * lax.rsqrt(jnp.mean(tok_float * tok_float, axis=-1, keepdims=True) + 1e-06)
    ).astype(jnp.bfloat16)
    for e in range(experts):
        chosen = jnp.logical_or(first == e, second == e)
        hot = jnp.logical_and(slot == rank[e : e + 1, :], chosen)
        select[e, :, :] = jnp.where(hot, 1.0, 0.0).astype(jnp.bfloat16)
        outgoing[e, :, :] = jnp.dot(
            select[e, :, :], normed, preferred_element_type=jnp.float32
        ).astype(jnp.bfloat16)

    for step in range(1, experts):
        token_copy(step).start()
    arrived[t] = outgoing[t]

    @pl.when(active)
    def _():
        for m in range(3):
            rows_buf[m, rows_at(me), :] = low[m, :, lanes_for(c)]
            for k in range(3):
                chip_back, core_back = quad_mates[k]
                source = 2 * lax.rem(chip_back, 2) + core_back
                pltpu.make_async_remote_copy(
                    src_ref=low.at[m, :, lanes_for(c)],
                    dst_ref=rows_buf.at[m, rows_at(source), :],
                    send_sem=quad_send.at[m, k],
                    recv_sem=quad_recv.at[m, source],
                    device_id=at(chip_back, core_back),
                    device_id_type=MESH,
                ).wait_recv()
            tile_buf[m, :, :] = rows_buf[m, :, :].T

            def send(n, _):
                i = lax.rem(n + turn_of(q), blocks)
                mine = is_mine(i)

                @pl.when(mine)
                def _():
                    outputs[m][:, place(q)] = tile_buf[m, block_rows(i), :]

                @pl.when(jnp.logical_not(mine))
                def _():
                    ring_copy(m, i).start()

                return 0

            lax.fori_loop(0, blocks, send, 0)


    chunk = 4 * LANES

    def turn(k, _):
        lanes = pl.ds(pl.multiple_of(k * chunk, chunk), chunk)
        tall = jnp.concatenate(
            [full[2, :, lanes], jnp.zeros((LANES - rows, chunk), jnp.float32)], axis=0
        )
        turned[lanes, :] = tall.T.astype(jnp.bfloat16)
        return 0

    lax.fori_loop(0, hidden // chunk, turn, 0)

    def pick(k, _):
        for p in range(2):
            picked[p, block_rows(k), :] = turned[block_rows(2 * k + p), :]
        return 0

    lax.fori_loop(0, half_ring, pick, 0)
    piece = 2 * LANES

    def lay(k, _):
        span = pl.ds(pl.multiple_of(k * piece, piece), piece)
        for p in range(2):
            split_down[p, :, span] = picked[p, span, :].T[:rows, :]
        return 0

    lax.fori_loop(0, hidden // 2 // piece, lay, 0)
    my_down[rows_at(c), :] = split_down[c]
    columns_copy = pltpu.make_async_remote_copy(
        src_ref=split_down.at[1 - c],
        dst_ref=my_down.at[rows_at(c), :],
        send_sem=core_send.at[0],
        recv_sem=core_recv.at[0],
        device_id=at(z, 1 - c),
        device_id_type=MESH,
    )
    columns_copy.start()

    def forward(m, j):
        other = expected_quad(j)

        @pl.when(jnp.logical_not(jnp.logical_and(own, other == q)))
        def _():
            unit_arrival(m, other).wait_recv()

        for step in range(1, groups):
            group_copy(m, j, step).start()

    def arrive(m):
        def body(index, _):
            here = jnp.logical_and(
                lax.rem(index, spread) == g // 2, lax.rem(index // spread, 2) == parity
            )

            @pl.when(jnp.logical_not(here))
            def _():
                unit_arrival(m, index).wait_recv()

            return 0

        lax.fori_loop(0, quads, body, 0)

    for m in range(2):

        def body(j, _):
            forward(m, j)
            return 0

        lax.fori_loop(0, own_count, body, 0)
    for m in range(2):
        arrive(m)
    for step in range(1, experts):
        token_arrival(step).wait_recv()

    wide = slots // 2

    def hide(k, _):
        own_tokens = arrived[pl.ds(k * (experts // 2), experts // 2)].reshape(wide, width)
        gated = lax.dot_general(gate_out[...], own_tokens, NT, preferred_element_type=jnp.float32)
        lifted = lax.dot_general(up_out[...], own_tokens, NT, preferred_element_type=jnp.float32)
        hidden_all[k, block_rows(pair), :] = (
            gated * (1.0 / (1.0 + jnp.exp(-gated))) * lifted
        ).astype(jnp.bfloat16)
        return 0

    lax.fori_loop(0, 2, hide, 0)

    part = wide // SUB

    def hop_copy(way, k, step, j):
        chip = lax.rem(z + chips - step if way == 0 else z + step, half_ring)
        return pltpu.make_async_remote_copy(
            src_ref=hidden_all.at[k, block_rows(chip), pl.ds(j * part, part)],
            dst_ref=hidden_all.at[k, block_rows(chip), pl.ds(j * part, part)],
            send_sem=hop_send.at[way, k, step, j],
            recv_sem=hop_recv.at[way, k, step, j],
            device_id=at(next_chip if way == 0 else last_chip, c),
            device_id_type=MESH,
        )

    def hop_arrival(way, k, step, j):
        chip = lax.rem(z + chips - step - 1 if way == 0 else z + step + 1, half_ring)
        return pltpu.make_async_remote_copy(
            src_ref=hidden_all.at[k, block_rows(chip), pl.ds(j * part, part)],
            dst_ref=hidden_all.at[k, block_rows(chip), pl.ds(j * part, part)],
            send_sem=hop_send.at[way, k, step, j],
            recv_sem=hop_recv.at[way, k, step, j],
            device_id=at(last_chip if way == 0 else next_chip, c),
            device_id_type=MESH,
        )

    for k in range(2):
        for j in range(SUB):
            for way in range(2):
                hop_copy(way, k, 0, j).start()

    def hop(step, _):
        @pl.when(step < own_count)
        def _():
            forward(2, step)

        for k in range(2):
            for j in range(SUB):
                for way in range(2):
                    hop_arrival(way, k, step, j).wait_recv()

                    @pl.when(jnp.logical_or(step < reach - 2, k == way))
                    def _():
                        hop_copy(way, k, step + 1, j).start()

        return 0

    lax.fori_loop(0, reach - 1, hop, 0)
    for j in range(reach - 1, own_count):
        forward(2, j)
    for way in range(2):
        for j in range(SUB):
            hop_arrival(way, way, reach - 1, j).wait_recv()
    columns_copy.wait()

    for k in range(2):
        partial[k, :, :] = jnp.dot(
            my_down[...], hidden_all[k, :, :], preferred_element_type=jnp.float32
        )

    partial_copy = pltpu.make_async_remote_copy(
        src_ref=partial.at[:, rows_at(1 - c), :],
        dst_ref=partial_in,
        send_sem=core_send.at[1],
        recv_sem=core_recv.at[1],
        device_id=at(z, 1 - c),
        device_id_type=MESH,
    )
    partial_copy.start()
    partial_copy.wait_recv()
    for e in range(experts):
        k, lane = e // (experts // 2), (e % (experts // 2)) * CAP
        lanes = pl.ds(lane, CAP)
        column_out[e, :, :] = (
            partial[k, rows_at(c), lanes] + partial_in[k, :, lanes]
        ).astype(jnp.bfloat16)

    def back_copy(step):
        other = lax.rem(t + step, experts)
        return pltpu.make_async_remote_copy(
            src_ref=column_out.at[other],
            dst_ref=returned.at[t],
            send_sem=back_send.at[step - 1],
            recv_sem=back_recv.at[t],
            device_id={"tp": other},
            device_id_type=MESH,
        )

    def back_arrival(step):
        other = lax.rem(t + step, experts)
        return pltpu.make_async_remote_copy(
            src_ref=column_out.at[other],
            dst_ref=returned.at[other],
            send_sem=back_send.at[step - 1],
            recv_sem=back_recv.at[other],
            device_id={"tp": other},
            device_id_type=MESH,
        )

    for step in range(1, experts):
        back_copy(step).start()
    returned[t] = column_out[t]
    for step in range(1, experts):
        back_arrival(step).wait_recv()
    total = jnp.zeros((rows, token_count), jnp.float32)
    for e in range(experts):
        weight = jnp.where(first == e, route_weight[0:1, :], 0.0) + jnp.where(
            second == e, route_weight[1:2, :], 0.0
        )
        total = total + weight * jnp.dot(
            returned[e, :, :], select[e, :, :], preferred_element_type=jnp.float32
        )
    mixed_out[...] = total.astype(jnp.bfloat16)

    arrive(2)
    for m in range(3):

        @pl.when(active)
        def _():
            for k in range(3):
                mate_copy(m, k).wait_send()

            def sent(i, _):
                @pl.when(jnp.logical_not(is_mine(i)))
                def _():
                    ring_copy(m, i).wait_send()

                return 0

            lax.fori_loop(0, blocks, sent, 0)

        def passed(j, _):
            for step in range(1, groups):
                group_copy(m, j, step).wait_send()
            return 0

        lax.fori_loop(0, own_count, passed, 0)

    def hopped(step, _):
        for k in range(2):
            for way in range(2):

                @pl.when(jnp.logical_or(step < reach - 1, k == way))
                def _():
                    for j in range(SUB):
                        hop_copy(way, k, step, j).wait_send()

        return 0

    lax.fori_loop(0, reach, hopped, 0)
    partial_copy.wait_send()
    for step in range(1, experts):
        token_copy(step).wait_send()
        back_copy(step).wait_send()


def layer(groups, chips, experts, *operands):
    tokens, gate = operands[3], operands[4]
    rows, hidden = gate.shape
    units = hidden // chips
    width = rows * 2 * chips
    quads = chips // 2
    share = hidden // 4
    reach = chips // 4
    wide = experts * CAP // 2
    served = jax.ShapeDtypeStruct((units, width), jnp.bfloat16)
    dma = pltpu.SemaphoreType.DMA
    return pl.pallas_call(
        functools.partial(layer_kernel, groups, chips, experts),
        out_shape=(
            served,
            served,
            served,
            jax.ShapeDtypeStruct((rows, tokens.shape[0]), jnp.bfloat16),
        ),
        in_specs=[pl.BlockSpec(memory_space=pltpu.VMEM)] * 3
        + [pl.BlockSpec(memory_space=pltpu.HBM)] * 4,
        out_specs=[pl.BlockSpec(memory_space=pltpu.VMEM)] * 4,
        scratch_shapes=[
            pltpu.VMEM(tokens.shape, jnp.bfloat16),
            pltpu.VMEM((3, rows, hidden), jnp.float32),
            pltpu.VMEM((3, rows, hidden), jnp.bfloat16),
            pltpu.VMEM((3, 4 * rows, share), jnp.bfloat16),
            pltpu.VMEM((3, share, 4 * rows), jnp.bfloat16),
            pltpu.VMEM((experts, CAP, tokens.shape[0]), jnp.bfloat16),
            pltpu.VMEM((experts, CAP, width), jnp.bfloat16),
            pltpu.VMEM((experts, CAP, width), jnp.bfloat16),
            pltpu.VMEM((hidden, LANES), jnp.bfloat16),
            pltpu.VMEM((2, hidden // 2, LANES), jnp.bfloat16),
            pltpu.VMEM((2, rows, hidden // 2), jnp.bfloat16),
            pltpu.VMEM((2 * rows, hidden // 2), jnp.bfloat16),
            pltpu.VMEM((2, hidden // 2, wide), jnp.bfloat16),
            pltpu.VMEM((2, 2 * rows, wide), jnp.float32),
            pltpu.VMEM((2, rows, wide), jnp.float32),
            pltpu.VMEM((experts, rows, CAP), jnp.bfloat16),
            pltpu.VMEM((experts, rows, CAP), jnp.bfloat16),
            dma((3, 3)),
            dma((3, 4)),
            dma((3, share // units)),
            dma((3, quads)),
            dma((3, quads // groups, groups - 1)),
            dma((experts - 1,)),
            dma((experts,)),
            dma((2,)),
            dma((2,)),
            dma((2, 2, reach, SUB)),
            dma((2, 2, reach, SUB)),
            dma((experts - 1,)),
            dma((experts,)),
            dma((4,)),
        ],
        compiler_params=pltpu.CompilerParams(
            collective_id=0, has_side_effects=True, vmem_limit_bytes=52736 * 1024
        ),
        name="layer",
    )(*operands)


def store_kernel(*refs):
    count = len(refs) // 2
    sem = refs[-1]
    copies = [
        pltpu.make_async_copy(refs[i], refs[count + i], sem.at[i]) for i in range(count)
    ]
    for copy in copies:
        copy.start()
    for copy in copies:
        copy.wait()


def stored(arrays):
    return pl.pallas_call(
        store_kernel,
        out_shape=tuple(jax.ShapeDtypeStruct(x.shape, x.dtype) for x in arrays),
        in_specs=[pl.BlockSpec(memory_space=pltpu.VMEM)] * len(arrays),
        out_specs=[pl.BlockSpec(memory_space=pltpu.HBM)] * len(arrays),
        scratch_shapes=[pltpu.SemaphoreType.DMA((len(arrays),))],
        compiler_params=pltpu.CompilerParams(vmem_limit_bytes=4 * 1024 * 1024),
        name="store",
    )(*arrays)


def shards(tokens, routes, route_weight, norm_gain, gate_train, up_train, down_train):
    results = layer(
        lax.axis_size("grp"),
        lax.axis_size("fs_0"),
        lax.axis_size("tp"),
        routes.T,
        route_weight.T,
        norm_gain[None, :],
        tokens,
        gate_train[0],
        up_train[0],
        down_train[0].T,
    )
    gate_new, up_new, down_new, mixed = stored(results)
    return (gate_new.T[None], up_new.T[None], down_new[None], mixed.T)


def solution(mesh):
    cores = 2
    split = Mesh(
        mesh.devices.reshape(
            mesh.shape["grp"], mesh.shape["fs"] // cores, cores, mesh.shape["tp"]
        ),
        ("grp", "fs_0", "fs_1", "tp"),
    )
    placed = (
        P(("grp", "tp"), None),
        P(("grp", "tp"), None),
        P(("grp", "tp"), None),
        P(FS),
        P("tp", FS, None),
        P("tp", FS, None),
        P("tp", None, FS),
    )
    return jax.shard_map(
        shards,
        mesh=split,
        in_specs=placed,
        out_specs=(
            P(("grp", "tp"), None, FS),
            P(("grp", "tp"), None, FS),
            P(("grp", "tp"), FS, None),
            P(("grp", "tp"), FS),
        ),
        check_vma=False,
    )
```

```python
import functools

import jax
import jax.numpy as jnp
from jax import lax
from jax.experimental import pallas as pl
from jax.experimental.pallas import tpu as pltpu
from jax.sharding import Mesh
from jax.sharding import PartitionSpec as P

CAP = 128
LANES = 128
FS = ("fs_0", "fs_1")
MESH = pl.DeviceIdType.MESH
SUB = 2
NT = (((1,), (1,)), ((), ()))


def layer_kernel(
    groups,
    chips,
    experts,
    routes,
    route_weight,
    gain,
    tokens_far,
    gate_far,
    up_far,
    down_far,
    gate_out,
    up_out,
    down_out,
    mixed_out,
    tokens,
    full,
    low,
    rows_buf,
    tile_buf,
    select,
    outgoing,
    arrived,
    split_down,
    my_down,
    hidden_all,
    partial,
    column_out,
    returned,
    quad_send,
    quad_recv,
    ring_send,
    unit_recv,
    group_send,
    token_send,
    token_recv,
    core_send,
    core_recv,
    hop_send,
    hop_recv,
    back_send,
    back_recv,
    read_sem,
):
    g = lax.axis_index("grp")
    z = lax.axis_index("fs_0")
    c = lax.axis_index("fs_1")
    t = lax.axis_index("tp")
    quads = chips // 2
    half_ring = chips // 2
    rows, hidden = gate_far.shape
    units = gate_out.shape[0]
    spread = groups // 2
    share = hidden // 4
    blocks = share // units
    own_count = quads // groups
    slots = experts * CAP
    q = z // 2
    odd = lax.rem(z, 2)
    me = 2 * odd + c
    half = lax.rem(g + q // spread, 2)
    active = lax.rem(q, spread) == g // 2
    pair = lax.rem(z, half_ring)
    my_block = 2 * pair + c
    my_half = my_block // (2 * blocks)
    my_source_core = lax.rem(my_block, 2 * blocks) // blocks
    parity = lax.rem(my_half + g, 2)
    own = jnp.logical_and(active, jnp.logical_and(half == my_half, c == my_source_core))
    outputs = (gate_out, up_out, down_out)
    reach = half_ring // 2

    def at(chip, core):
        return {"fs_0": chip, "fs_1": core}

    def own_quad(j):
        return spread * (2 * j + parity) + g // 2

    def listed(m, n):
        if m == 1:
            return jnp.where(lax.rem(q // (2 * spread), 2) == 1, blocks - 1 - n, n)
        return n

    def expected_quad(m, n):
        if m == 1 and own_count > 1:
            early = lax.rem(my_block, blocks) >= blocks // 2
            wanted = own_count // 2
            first_half = n < wanted
            odd_turn = jnp.logical_xor(early, jnp.logical_not(first_half))
            within = jnp.where(first_half, n, n - wanted)
            return own_quad(2 * within + jnp.where(odd_turn, 1, 0))
        return own_quad(n)

    def sender_of(other):
        right = lax.rem(z - (2 * other + 1) + chips, chips) < half_ring
        return 2 * other + jnp.where(right, 1, 0)

    def target(i):
        chip = half * blocks + c * (blocks // 2) + i // 2
        right = lax.rem(chip - z + 2 * chips, half_ring)
        left = lax.rem(z - chip + 2 * chips, half_ring)
        chip = jnp.where(odd == 1, z + right, z - left + chips)
        return lax.rem(chip, chips), lax.rem(i, 2)

    def place(index):
        return pl.ds(pl.multiple_of(index * LANES, LANES), LANES)

    def block_rows(index):
        return pl.ds(pl.multiple_of(index * units, 16), units)

    def rows_at(index):
        return pl.ds(pl.multiple_of(index * rows, rows), rows)

    quad_mates = ((z + 1 - 2 * odd, c), (z, 1 - c), (z + 1 - 2 * odd, 1 - c))
    next_chip = lax.rem(z + 1, chips)
    last_chip = lax.rem(z + chips - 1, chips)

    reads = [
        pltpu.make_async_copy(far, full.at[m], read_sem.at[m])
        for m, far in enumerate((gate_far, up_far, down_far))
    ]
    reads.append(pltpu.make_async_copy(tokens_far, tokens, read_sem.at[3]))
    for read in reads:
        read.start()

    barrier = pltpu.get_barrier_semaphore()

    def greet_device(where):
        pl.semaphore_signal(barrier, inc=1, device_id=where, device_id_type=MESH)

    def greet(j, _):
        other = own_quad(j)
        chip = sender_of(other)

        @pl.when(jnp.logical_not(jnp.logical_and(own, other == q)))
        def _():
            greet_device(at(chip, my_source_core))

        return 0

    lax.fori_loop(0, own_count, greet, 0)
    for chip, core in quad_mates:
        greet_device(at(chip, core))
    for step in range(1, groups):
        greet_device({"grp": lax.rem(g + step, groups)})
    for step in range(1, experts):
        for core in range(2):
            greet_device({"tp": lax.rem(t + step, experts), "fs_1": core})
    greet_device(at(next_chip, c))
    greet_device(at(last_chip, c))

    eye = lax.broadcasted_iota(jnp.int32, (rows, rows), 0) == lax.broadcasted_iota(
        jnp.int32, (rows, rows), 1
    )
    gain_column = jnp.sum(jnp.where(eye, gain[...], 0.0), axis=1, keepdims=True)
    for m in range(2):
        reads[m].wait()
        low[m, :, :] = (full[m] * gain_column).astype(jnp.bfloat16)
    reads[2].wait()
    low[2, :, :] = full[2].astype(jnp.bfloat16)

    expected = jnp.where(active, blocks - jnp.where(own, 1, 0), 0)
    pl.semaphore_wait(barrier, expected + groups - 1 + 3 + 2 * (experts - 1) + 2)

    def lanes_for(core):
        return pl.ds(pl.multiple_of((2 * half + core) * share, LANES), share)

    def mate_copy(m, k):
        chip, core = quad_mates[k]
        return pltpu.make_async_remote_copy(
            src_ref=low.at[m, :, lanes_for(core)],
            dst_ref=rows_buf.at[m, rows_at(me), :],
            send_sem=quad_send.at[m, k],
            recv_sem=quad_recv.at[m, me],
            device_id=at(chip, core),
            device_id_type=MESH,
        )

    def ring_copy(m, i):
        chip, core = target(i)
        return pltpu.make_async_remote_copy(
            src_ref=tile_buf.at[m, block_rows(i), :],
            dst_ref=outputs[m].at[:, place(q)],
            send_sem=ring_send.at[m, i],
            recv_sem=unit_recv.at[m, q],
            device_id=at(chip, core),
            device_id_type=MESH,
        )

    def group_copy(m, j, step):
        other = expected_quad(m, j)
        return pltpu.make_async_remote_copy(
            src_ref=outputs[m].at[:, place(other)],
            dst_ref=outputs[m].at[:, place(other)],
            send_sem=group_send.at[m, j, step - 1],
            recv_sem=unit_recv.at[m, other],
            device_id={"grp": lax.rem(g + step, groups)},
            device_id_type=MESH,
        )

    def unit_arrival(m, index):
        return pltpu.make_async_remote_copy(
            src_ref=outputs[m].at[:, place(index)],
            dst_ref=outputs[m].at[:, place(index)],
            send_sem=group_send.at[m, 0, 0],
            recv_sem=unit_recv.at[m, index],
            device_id={"grp": lax.rem(g + 1, groups)},
            device_id_type=MESH,
        )

    def is_mine(i):
        chip, core = target(i)
        return jnp.logical_and(chip == z, core == c)

    def token_copy(step):
        other = lax.rem(t + step, experts)
        return pltpu.make_async_remote_copy(
            src_ref=outgoing.at[other],
            dst_ref=arrived.at[t],
            send_sem=token_send.at[step - 1],
            recv_sem=token_recv.at[t],
            device_id={"tp": other},
            device_id_type=MESH,
        )

    def token_arrival(step):
        other = lax.rem(t + step, experts)
        return pltpu.make_async_remote_copy(
            src_ref=outgoing.at[other],
            dst_ref=arrived.at[other],
            send_sem=token_send.at[step - 1],
            recv_sem=token_recv.at[other],
            device_id={"tp": other},
            device_id_type=MESH,
        )

    @pl.when(active)
    def _():
        for m in range(3):
            for k in range(3):
                mate_copy(m, k).start()

    token_count, width = tokens.shape
    first = routes[0:1, :]
    second = routes[1:2, :]
    expert_row = lax.broadcasted_iota(jnp.int32, (8, token_count), 0)
    named = jnp.logical_or(first == expert_row, second == expert_row)
    before = (
        lax.broadcasted_iota(jnp.int32, (token_count, token_count), 0)
        < lax.broadcasted_iota(jnp.int32, (token_count, token_count), 1)
    )
    rank = jnp.dot(
        jnp.where(named, 1.0, 0.0).astype(jnp.bfloat16),
        jnp.where(before, 1.0, 0.0).astype(jnp.bfloat16),
        preferred_element_type=jnp.float32,
    )
    slot = lax.broadcasted_iota(jnp.int32, (CAP, token_count), 0).astype(jnp.float32)
    reads[3].wait()
    tok_float = tokens[...].astype(jnp.float32)
    normed = (
        tok_float * lax.rsqrt(jnp.mean(tok_float * tok_float, axis=-1, keepdims=True) + 1e-06)
    ).astype(jnp.bfloat16)
    for e in range(experts):
        chosen = jnp.logical_or(first == e, second == e)
        hot = jnp.logical_and(slot == rank[e : e + 1, :], chosen)
        select[e, :, :] = jnp.where(hot, 1.0, 0.0).astype(jnp.bfloat16)
        outgoing[e, :, :] = jnp.dot(
            select[e, :, :], normed, preferred_element_type=jnp.float32
        ).astype(jnp.bfloat16)

    for step in range(1, experts):
        token_copy(step).start()
    arrived[t] = outgoing[t]

    @pl.when(active)
    def _():
        for m in range(3):
            rows_buf[m, rows_at(me), :] = low[m, :, lanes_for(c)]
            for k in range(3):
                chip_back, core_back = quad_mates[k]
                source = 2 * lax.rem(chip_back, 2) + core_back
                pltpu.make_async_remote_copy(
                    src_ref=low.at[m, :, lanes_for(c)],
                    dst_ref=rows_buf.at[m, rows_at(source), :],
                    send_sem=quad_send.at[m, k],
                    recv_sem=quad_recv.at[m, source],
                    device_id=at(chip_back, core_back),
                    device_id_type=MESH,
                ).wait_recv()
            tile_buf[m, :, :] = rows_buf[m, :, :].T

            def send(n, _):
                i = listed(m, n)
                mine = is_mine(i)

                @pl.when(mine)
                def _():
                    outputs[m][:, place(q)] = tile_buf[m, block_rows(i), :]

                @pl.when(jnp.logical_not(mine))
                def _():
                    ring_copy(m, i).start()

                return 0

            lax.fori_loop(0, blocks, send, 0)


    for k in range(half_ring):
        for p in range(2):
            start = (2 * k + p) * units
            split_down[p, k, :, :] = low[2, :, start : start + units]
    for k in range(half_ring):
        my_down[k, rows_at(c), :] = split_down[c, k]
    columns_copy = pltpu.make_async_remote_copy(
        src_ref=split_down.at[1 - c],
        dst_ref=my_down.at[:, rows_at(c), :],
        send_sem=core_send.at[0],
        recv_sem=core_recv.at[0],
        device_id=at(z, 1 - c),
        device_id_type=MESH,
    )
    columns_copy.start()

    def forward(m, j):
        other = expected_quad(m, j)

        @pl.when(jnp.logical_not(jnp.logical_and(own, other == q)))
        def _():
            unit_arrival(m, other).wait_recv()

        for step in range(1, groups):
            group_copy(m, j, step).start()

    def arrive(m):
        def body(index, _):
            here = jnp.logical_and(
                lax.rem(index, spread) == g // 2, lax.rem(index // spread, 2) == parity
            )

            @pl.when(jnp.logical_not(here))
            def _():
                unit_arrival(m, index).wait_recv()

            return 0

        lax.fori_loop(0, quads, body, 0)

    for m in range(2):

        def body(j, _):
            forward(m, j)
            return 0

        lax.fori_loop(0, own_count, body, 0)
    for m in range(2):
        arrive(m)
    for step in range(1, experts):
        token_arrival(step).wait_recv()

    wide = slots // 2

    def hide(k):
        own_tokens = arrived[k * (experts // 2) : (k + 1) * (experts // 2)].reshape(wide, width)
        gated = lax.dot_general(gate_out[...], own_tokens, NT, preferred_element_type=jnp.float32)
        lifted = lax.dot_general(up_out[...], own_tokens, NT, preferred_element_type=jnp.float32)
        hidden_all[k, block_rows(pair), :] = (
            gated * (1.0 / (1.0 + jnp.exp(-gated))) * lifted
        ).astype(jnp.bfloat16)

    part = wide // SUB

    def hop_copy(way, k, step, j):
        chip = lax.rem(z + chips - step if way == 0 else z + step, half_ring)
        return pltpu.make_async_remote_copy(
            src_ref=hidden_all.at[k, block_rows(chip), pl.ds(j * part, part)],
            dst_ref=hidden_all.at[k, block_rows(chip), pl.ds(j * part, part)],
            send_sem=hop_send.at[way, k, step, j],
            recv_sem=hop_recv.at[way, k, step, j],
            device_id=at(next_chip if way == 0 else last_chip, c),
            device_id_type=MESH,
        )

    def hop_arrival(way, k, step, j):
        chip = lax.rem(z + chips - step - 1 if way == 0 else z + step + 1, half_ring)
        return pltpu.make_async_remote_copy(
            src_ref=hidden_all.at[k, block_rows(chip), pl.ds(j * part, part)],
            dst_ref=hidden_all.at[k, block_rows(chip), pl.ds(j * part, part)],
            send_sem=hop_send.at[way, k, step, j],
            recv_sem=hop_recv.at[way, k, step, j],
            device_id=at(last_chip if way == 0 else next_chip, c),
            device_id_type=MESH,
        )

    def add_block(k, chip, fresh=False):
        term = jnp.dot(
            my_down[chip], hidden_all[k, block_rows(chip), :], preferred_element_type=jnp.float32
        )
        partial[k, :, :] = term if fresh else partial[k, :, :] + term

    for k in range(2):
        hide(k)
        for j in range(SUB):
            for way in range(2):
                hop_copy(way, k, 0, j).start()
    columns_copy.wait()
    for k in range(2):
        add_block(k, pair, True)

    def source_of(way, step):
        return lax.rem(z + chips - step - 1 if way == 0 else z + step + 1, half_ring)

    def hop(step, _):
        @pl.when(step < own_count)
        def _():
            forward(2, step)

        for k in range(2):
            for j in range(SUB):
                for way in range(2):
                    hop_arrival(way, k, step, j).wait_recv()

                    @pl.when(jnp.logical_or(step < reach - 2, k == way))
                    def _():
                        hop_copy(way, k, step + 1, j).start()

        for k in range(2):
            for way in range(2):
                add_block(k, source_of(way, step))
        return 0

    lax.fori_loop(0, reach - 1, hop, 0)
    for j in range(reach - 1, own_count):
        forward(2, j)
    for way in range(2):
        for j in range(SUB):
            hop_arrival(way, way, reach - 1, j).wait_recv()
    for k in range(2):
        add_block(k, source_of(k, reach - 1))

    def back_copy(step, core):
        other = lax.rem(t + step, experts)
        return pltpu.make_async_remote_copy(
            src_ref=column_out.at[other, rows_at(core), :],
            dst_ref=returned.at[t, c],
            send_sem=back_send.at[step, core],
            recv_sem=back_recv.at[t, c],
            device_id={"tp": other, "fs_1": core},
            device_id_type=MESH,
        )

    def back_arrival(step, core):
        other = lax.rem(t + step, experts)
        return pltpu.make_async_remote_copy(
            src_ref=column_out.at[other, rows_at(c), :],
            dst_ref=returned.at[other, core],
            send_sem=back_send.at[step, core],
            recv_sem=back_recv.at[other, core],
            device_id={"tp": other, "fs_1": core},
            device_id_type=MESH,
        )

    for e in range(experts):
        k, lane = e // (experts // 2), (e % (experts // 2)) * CAP
        column_out[e, :, :] = partial[k, :, lane : lane + CAP]
    for step in range(1, experts):
        for core in range(2):
            back_copy(step, core).start()
    back_copy(0, 1 - c).start()
    returned[t, c] = column_out[t, rows_at(c), :]
    back_arrival(0, 1 - c).wait_recv()
    for step in range(1, experts):
        for core in range(2):
            back_arrival(step, core).wait_recv()
    total = jnp.zeros((rows, token_count), jnp.float32)
    for e in range(experts):
        weight = jnp.where(first == e, route_weight[0:1, :], 0.0) + jnp.where(
            second == e, route_weight[1:2, :], 0.0
        )
        total = total + weight * jnp.dot(
            (returned[e, 0] + returned[e, 1]).astype(jnp.bfloat16),
            select[e, :, :],
            preferred_element_type=jnp.float32,
        )
    mixed_out[...] = total.astype(jnp.bfloat16)

    arrive(2)
    for m in range(3):

        @pl.when(active)
        def _():
            for k in range(3):
                mate_copy(m, k).wait_send()

            def sent(i, _):
                @pl.when(jnp.logical_not(is_mine(i)))
                def _():
                    ring_copy(m, i).wait_send()

                return 0

            lax.fori_loop(0, blocks, sent, 0)

        def passed(j, _):
            for step in range(1, groups):
                group_copy(m, j, step).wait_send()
            return 0

        lax.fori_loop(0, own_count, passed, 0)

    def hopped(step, _):
        for k in range(2):
            for way in range(2):

                @pl.when(jnp.logical_or(step < reach - 1, k == way))
                def _():
                    for j in range(SUB):
                        hop_copy(way, k, step, j).wait_send()

        return 0

    lax.fori_loop(0, reach, hopped, 0)
    for step in range(1, experts):
        token_copy(step).wait_send()
        for core in range(2):
            back_copy(step, core).wait_send()
    back_copy(0, 1 - c).wait_send()


def layer(groups, chips, experts, *operands):
    tokens, gate = operands[3], operands[4]
    rows, hidden = gate.shape
    units = hidden // chips
    width = rows * 2 * chips
    quads = chips // 2
    share = hidden // 4
    reach = chips // 4
    wide = experts * CAP // 2
    served = jax.ShapeDtypeStruct((units, width), jnp.bfloat16)
    dma = pltpu.SemaphoreType.DMA
    return pl.pallas_call(
        functools.partial(layer_kernel, groups, chips, experts),
        out_shape=(
            served,
            served,
            served,
            jax.ShapeDtypeStruct((rows, tokens.shape[0]), jnp.bfloat16),
        ),
        in_specs=[pl.BlockSpec(memory_space=pltpu.VMEM)] * 3
        + [pl.BlockSpec(memory_space=pltpu.HBM)] * 4,
        out_specs=[pl.BlockSpec(memory_space=pltpu.VMEM)] * 4,
        scratch_shapes=[
            pltpu.VMEM(tokens.shape, jnp.bfloat16),
            pltpu.VMEM((3, rows, hidden), jnp.float32),
            pltpu.VMEM((3, rows, hidden), jnp.bfloat16),
            pltpu.VMEM((3, 4 * rows, share), jnp.bfloat16),
            pltpu.VMEM((3, share, 4 * rows), jnp.bfloat16),
            pltpu.VMEM((experts, CAP, tokens.shape[0]), jnp.bfloat16),
            pltpu.VMEM((experts, CAP, width), jnp.bfloat16),
            pltpu.VMEM((experts, CAP, width), jnp.bfloat16),
            pltpu.VMEM((2, chips // 2, rows, units), jnp.bfloat16),
            pltpu.VMEM((chips // 2, 2 * rows, units), jnp.bfloat16),
            pltpu.VMEM((2, hidden // 2, wide), jnp.bfloat16),
            pltpu.VMEM((2, 2 * rows, wide), jnp.float32),
            pltpu.VMEM((experts, 2 * rows, CAP), jnp.float32),
            pltpu.VMEM((experts, 2, rows, CAP), jnp.float32),
            dma((3, 3)),
            dma((3, 4)),
            dma((3, share // units)),
            dma((3, quads)),
            dma((3, quads // groups, groups - 1)),
            dma((experts - 1,)),
            dma((experts,)),
            dma((1,)),
            dma((1,)),
            dma((2, 2, reach, SUB)),
            dma((2, 2, reach, SUB)),
            dma((experts, 2)),
            dma((experts, 2)),
            dma((4,)),
        ],
        compiler_params=pltpu.CompilerParams(
            collective_id=0, has_side_effects=True, vmem_limit_bytes=52736 * 1024
        ),
        name="layer",
    )(*operands)


def store_kernel(*refs):
    count = len(refs) // 2
    sem = refs[-1]
    copies = [
        pltpu.make_async_copy(refs[i], refs[count + i], sem.at[i]) for i in range(count)
    ]
    for copy in copies:
        copy.start()
    for copy in copies:
        copy.wait()


def stored(arrays):
    return pl.pallas_call(
        store_kernel,
        out_shape=tuple(jax.ShapeDtypeStruct(x.shape, x.dtype) for x in arrays),
        in_specs=[pl.BlockSpec(memory_space=pltpu.VMEM)] * len(arrays),
        out_specs=[pl.BlockSpec(memory_space=pltpu.HBM)] * len(arrays),
        scratch_shapes=[pltpu.SemaphoreType.DMA((len(arrays),))],
        compiler_params=pltpu.CompilerParams(vmem_limit_bytes=4 * 1024 * 1024),
        name="store",
    )(*arrays)


def shards(tokens, routes, route_weight, norm_gain, gate_train, up_train, down_train):
    results = layer(
        lax.axis_size("grp"),
        lax.axis_size("fs_0"),
        lax.axis_size("tp"),
        routes.T,
        route_weight.T,
        norm_gain[None, :],
        tokens,
        gate_train[0],
        up_train[0],
        down_train[0].T,
    )
    gate_new, up_new, down_new, mixed = stored(results)
    return (gate_new.T[None], up_new.T[None], down_new[None], mixed.T)


def solution(mesh):
    cores = 2
    split = Mesh(
        mesh.devices.reshape(
            mesh.shape["grp"], mesh.shape["fs"] // cores, cores, mesh.shape["tp"]
        ),
        ("grp", "fs_0", "fs_1", "tp"),
    )
    placed = (
        P(("grp", "tp"), None),
        P(("grp", "tp"), None),
        P(("grp", "tp"), None),
        P(FS),
        P("tp", FS, None),
        P("tp", FS, None),
        P("tp", None, FS),
    )
    return jax.shard_map(
        shards,
        mesh=split,
        in_specs=placed,
        out_specs=(
            P(("grp", "tp"), None, FS),
            P(("grp", "tp"), None, FS),
            P(("grp", "tp"), FS, None),
            P(("grp", "tp"), FS),
        ),
        check_vma=False,
    )
```

```python
import functools

import jax
import jax.numpy as jnp
from jax import lax
from jax.experimental import pallas as pl
from jax.experimental.pallas import tpu as pltpu
from jax.sharding import Mesh
from jax.sharding import PartitionSpec as P

CAP = 128
LANES = 128
FS = ("fs_0", "fs_1")
MESH = pl.DeviceIdType.MESH
SUB = 2
NT = (((1,), (1,)), ((), ()))


def layer_kernel(
    groups,
    chips,
    experts,
    routes,
    route_weight,
    gain,
    tokens_far,
    gate_far,
    up_far,
    down_far,
    gate_out,
    up_out,
    down_out,
    mixed_out,
    tokens,
    full,
    low,
    rows_buf,
    tile_buf,
    select,
    outgoing,
    arrived,
    split_down,
    my_down,
    hidden_all,
    partial,
    column_out,
    returned,
    quad_send,
    quad_recv,
    ring_send,
    unit_recv,
    group_send,
    token_send,
    token_recv,
    core_send,
    core_recv,
    hop_send,
    hop_recv,
    back_send,
    back_recv,
    read_sem,
    ready,
):
    g = lax.axis_index("grp")
    z = lax.axis_index("fs_0")
    c = lax.axis_index("fs_1")
    t = lax.axis_index("tp")
    quads = chips // 2
    half_ring = chips // 2
    rows, hidden = gate_far.shape
    units = gate_out.shape[0]
    spread = groups // 2
    share = hidden // 4
    blocks = share // units
    own_count = quads // groups
    slots = experts * CAP
    q = z // 2
    odd = lax.rem(z, 2)
    me = 2 * odd + c
    half = lax.rem(g + q // spread, 2)
    active = lax.rem(q, spread) == g // 2
    pair = lax.rem(z, half_ring)
    my_block = 2 * pair + c
    my_half = my_block // (2 * blocks)
    my_source_core = lax.rem(my_block, 2 * blocks) // blocks
    parity = lax.rem(my_half + g, 2)
    own = jnp.logical_and(active, jnp.logical_and(half == my_half, c == my_source_core))
    outputs = (gate_out, up_out, down_out)
    reach = half_ring // 2

    def at(chip, core):
        return {"fs_0": chip, "fs_1": core}

    def own_quad(j):
        return spread * (2 * j + parity) + g // 2

    def listed(m, n):
        if m == 1:
            return jnp.where(lax.rem(q // (2 * spread), 2) == 1, blocks - 1 - n, n)
        return lax.rem(n + c * (blocks // 2), blocks)

    def expected_quad(m, n):
        if m == 1 and own_count > 1:
            early = lax.rem(my_block, blocks) >= blocks // 2
            wanted = own_count // 2
            first_half = n < wanted
            odd_turn = jnp.logical_xor(early, jnp.logical_not(first_half))
            within = jnp.where(first_half, n, n - wanted)
            return own_quad(2 * within + jnp.where(odd_turn, 1, 0))
        return own_quad(n)

    def target(i):
        chip = half * blocks + c * (blocks // 2) + i // 2
        right = lax.rem(chip - z + 2 * chips, half_ring)
        left = lax.rem(z - chip + 2 * chips, half_ring)
        chip = jnp.where(odd == 1, z + right, z - left + chips)
        return lax.rem(chip, chips), lax.rem(i, 2)

    def place(index):
        return pl.ds(pl.multiple_of(index * LANES, LANES), LANES)

    def block_rows(index):
        return pl.ds(pl.multiple_of(index * units, 16), units)

    def rows_at(index):
        return pl.ds(pl.multiple_of(index * rows, rows), rows)

    quad_mates = ((z + 1 - 2 * odd, c), (z, 1 - c), (z + 1 - 2 * odd, 1 - c))
    next_chip = lax.rem(z + 1, chips)
    last_chip = lax.rem(z + chips - 1, chips)

    reads = [
        pltpu.make_async_copy(far, full.at[m], read_sem.at[m])
        for m, far in enumerate((gate_far, up_far, down_far))
    ]
    reads.append(pltpu.make_async_copy(tokens_far, tokens, read_sem.at[3]))
    for read in reads:
        read.start()

    barrier = pltpu.get_barrier_semaphore()

    def greet_device(where):
        pl.semaphore_signal(barrier, inc=1, device_id=where, device_id_type=MESH)

    for k in range(reach // 2):
        for core in range(2):
            greet_device(at(lax.rem(z + chips - (2 * k + 1 + odd), chips), core))
            greet_device(at(lax.rem(z + 2 * k + 2 - odd, chips), core))
    ahead = lax.rem(jnp.where(odd == 1, z + reach, z + chips - reach), chips)
    behind = lax.rem(jnp.where(odd == 1, z + chips - reach, z + reach), chips)
    greet_device(at(ahead, c))
    for chip, core in quad_mates:
        greet_device(at(chip, core))
    for step in range(1, groups):
        greet_device({"grp": lax.rem(g + step, groups)})
    for step in range(1, experts):
        for core in range(2):
            greet_device({"tp": lax.rem(t + step, experts), "fs_1": core})
    greet_device(at(next_chip, c))
    greet_device(at(last_chip, c))

    eye = lax.broadcasted_iota(jnp.int32, (rows, rows), 0) == lax.broadcasted_iota(
        jnp.int32, (rows, rows), 1
    )
    gain_column = jnp.sum(jnp.where(eye, gain[...], 0.0), axis=1, keepdims=True)
    for m in range(2):
        reads[m].wait()
        low[m, :, :] = (full[m] * gain_column).astype(jnp.bfloat16)
    reads[2].wait()
    low[2, :, :] = full[2].astype(jnp.bfloat16)

    pl.semaphore_wait(barrier, groups - 1 + 3 + 2 * (experts - 1) + 2 + 2 * reach + 1)

    def lanes_for(core):
        return pl.ds(pl.multiple_of((2 * half + core) * share, LANES), share)

    def mate_copy(m, k):
        chip, core = quad_mates[k]
        return pltpu.make_async_remote_copy(
            src_ref=low.at[m, :, lanes_for(core)],
            dst_ref=rows_buf.at[m, rows_at(me), :],
            send_sem=quad_send.at[m, k],
            recv_sem=quad_recv.at[m, me],
            device_id=at(chip, core),
            device_id_type=MESH,
        )

    def ring_copy(m, i):
        chip, core = target(i)
        return pltpu.make_async_remote_copy(
            src_ref=tile_buf.at[m, block_rows(i), :],
            dst_ref=outputs[m].at[:, place(q)],
            send_sem=ring_send.at[m, i],
            recv_sem=unit_recv.at[m, q],
            device_id=at(chip, core),
            device_id_type=MESH,
        )

    def group_copy(m, j, step):
        other = expected_quad(m, j)
        return pltpu.make_async_remote_copy(
            src_ref=outputs[m].at[:, place(other)],
            dst_ref=outputs[m].at[:, place(other)],
            send_sem=group_send.at[m, j, step - 1],
            recv_sem=unit_recv.at[m, other],
            device_id={"grp": lax.rem(g + step, groups)},
            device_id_type=MESH,
        )

    def unit_arrival(m, index):
        return pltpu.make_async_remote_copy(
            src_ref=outputs[m].at[:, place(index)],
            dst_ref=outputs[m].at[:, place(index)],
            send_sem=group_send.at[m, 0, 0],
            recv_sem=unit_recv.at[m, index],
            device_id={"grp": lax.rem(g + 1, groups)},
            device_id_type=MESH,
        )

    def is_near(i):
        chip, _ = target(i)
        away = lax.rem(jnp.where(odd == 1, chip - z, z - chip) + chips, chips)
        return away <= reach

    def is_mine(i):
        chip, core = target(i)
        return jnp.logical_and(chip == z, core == c)

    def send_tile(m, i):
        mine = is_mine(i)

        @pl.when(mine)
        def _():
            outputs[m][:, place(q)] = tile_buf[m, block_rows(i), :]

        @pl.when(jnp.logical_not(mine))
        def _():
            ring_copy(m, i).start()

    def token_copy(step):
        other = lax.rem(t + step, experts)
        return pltpu.make_async_remote_copy(
            src_ref=outgoing.at[other],
            dst_ref=arrived.at[t],
            send_sem=token_send.at[step - 1],
            recv_sem=token_recv.at[t],
            device_id={"tp": other},
            device_id_type=MESH,
        )

    def token_arrival(step):
        other = lax.rem(t + step, experts)
        return pltpu.make_async_remote_copy(
            src_ref=outgoing.at[other],
            dst_ref=arrived.at[other],
            send_sem=token_send.at[step - 1],
            recv_sem=token_recv.at[other],
            device_id={"tp": other},
            device_id_type=MESH,
        )

    @pl.when(active)
    def _():
        for m in range(3):
            for k in range(3):
                mate_copy(m, k).start()

    pl.semaphore_signal(ready, inc=1, device_id=at(behind, c), device_id_type=MESH)

    token_count, width = tokens.shape
    first = routes[0:1, :]
    second = routes[1:2, :]
    expert_row = lax.broadcasted_iota(jnp.int32, (8, token_count), 0)
    named = jnp.logical_or(first == expert_row, second == expert_row)
    before = (
        lax.broadcasted_iota(jnp.int32, (token_count, token_count), 0)
        < lax.broadcasted_iota(jnp.int32, (token_count, token_count), 1)
    )
    rank = jnp.dot(
        jnp.where(named, 1.0, 0.0).astype(jnp.bfloat16),
        jnp.where(before, 1.0, 0.0).astype(jnp.bfloat16),
        preferred_element_type=jnp.float32,
    )
    slot = lax.broadcasted_iota(jnp.int32, (CAP, token_count), 0).astype(jnp.float32)
    reads[3].wait()
    tok_float = tokens[...].astype(jnp.float32)
    normed = (
        tok_float * lax.rsqrt(jnp.mean(tok_float * tok_float, axis=-1, keepdims=True) + 1e-06)
    ).astype(jnp.bfloat16)
    for e in range(experts):
        chosen = jnp.logical_or(first == e, second == e)
        hot = jnp.logical_and(slot == rank[e : e + 1, :], chosen)
        select[e, :, :] = jnp.where(hot, 1.0, 0.0).astype(jnp.bfloat16)
        outgoing[e, :, :] = jnp.dot(
            select[e, :, :], normed, preferred_element_type=jnp.float32
        ).astype(jnp.bfloat16)

    for step in range(1, experts):
        token_copy(step).start()
    arrived[t] = outgoing[t]

    @pl.when(active)
    def _():
        for m in range(3):
            rows_buf[m, rows_at(me), :] = low[m, :, lanes_for(c)]
            for k in range(3):
                chip_back, core_back = quad_mates[k]
                source = 2 * lax.rem(chip_back, 2) + core_back
                pltpu.make_async_remote_copy(
                    src_ref=low.at[m, :, lanes_for(c)],
                    dst_ref=rows_buf.at[m, rows_at(source), :],
                    send_sem=quad_send.at[m, k],
                    recv_sem=quad_recv.at[m, source],
                    device_id=at(chip_back, core_back),
                    device_id_type=MESH,
                ).wait_recv()
            tile_buf[m, :, :] = rows_buf[m, :, :].T

            def send(n, _):
                send_tile(m, listed(m, n))
                return 0

            def send_if(near, n, _):
                @pl.when(is_near(n) == near)
                def _():
                    send_tile(m, n)

                return 0

            if m == 0:
                pl.semaphore_wait(ready, 1)
            lax.fori_loop(0, blocks, send, 0)

    @pl.when(jnp.logical_not(active))
    def _():
        pl.semaphore_wait(ready, 1)


    for k in range(half_ring):
        for p in range(2):
            start = (2 * k + p) * units
            split_down[p, k, :, :] = low[2, :, start : start + units]
    for k in range(half_ring):
        my_down[k, rows_at(c), :] = split_down[c, k]
    columns_copy = pltpu.make_async_remote_copy(
        src_ref=split_down.at[1 - c],
        dst_ref=my_down.at[:, rows_at(c), :],
        send_sem=core_send.at[0],
        recv_sem=core_recv.at[0],
        device_id=at(z, 1 - c),
        device_id_type=MESH,
    )
    columns_copy.start()

    def forward(m, j):
        other = expected_quad(m, j)

        @pl.when(jnp.logical_not(jnp.logical_and(own, other == q)))
        def _():
            unit_arrival(m, other).wait_recv()

        for step in range(1, groups):
            group_copy(m, j, step).start()

    def arrive(m):
        def body(index, _):
            here = jnp.logical_and(
                lax.rem(index, spread) == g // 2, lax.rem(index // spread, 2) == parity
            )

            @pl.when(jnp.logical_not(here))
            def _():
                unit_arrival(m, index).wait_recv()

            return 0

        lax.fori_loop(0, quads, body, 0)

    for m in range(2):

        def body(j, _):
            forward(m, j)
            return 0

        lax.fori_loop(0, own_count, body, 0)
    for m in range(2):
        arrive(m)
    for step in range(1, experts):
        token_arrival(step).wait_recv()

    wide = slots // 2

    def hide(k):
        own_tokens = arrived[k * (experts // 2) : (k + 1) * (experts // 2)].reshape(wide, width)
        gated = lax.dot_general(gate_out[...], own_tokens, NT, preferred_element_type=jnp.float32)
        lifted = lax.dot_general(up_out[...], own_tokens, NT, preferred_element_type=jnp.float32)
        hidden_all[k, block_rows(pair), :] = (
            gated * (1.0 / (1.0 + jnp.exp(-gated))) * lifted
        ).astype(jnp.bfloat16)

    part = wide // SUB

    def hop_copy(way, k, step, j):
        chip = lax.rem(z + chips - step if way == 0 else z + step, half_ring)
        return pltpu.make_async_remote_copy(
            src_ref=hidden_all.at[k, block_rows(chip), pl.ds(j * part, part)],
            dst_ref=hidden_all.at[k, block_rows(chip), pl.ds(j * part, part)],
            send_sem=hop_send.at[way, k, step, j],
            recv_sem=hop_recv.at[way, k, step, j],
            device_id=at(next_chip if way == 0 else last_chip, c),
            device_id_type=MESH,
        )

    def hop_arrival(way, k, step, j):
        chip = lax.rem(z + chips - step - 1 if way == 0 else z + step + 1, half_ring)
        return pltpu.make_async_remote_copy(
            src_ref=hidden_all.at[k, block_rows(chip), pl.ds(j * part, part)],
            dst_ref=hidden_all.at[k, block_rows(chip), pl.ds(j * part, part)],
            send_sem=hop_send.at[way, k, step, j],
            recv_sem=hop_recv.at[way, k, step, j],
            device_id=at(last_chip if way == 0 else next_chip, c),
            device_id_type=MESH,
        )

    def add_block(k, chip, fresh=False):
        term = jnp.dot(
            my_down[chip], hidden_all[k, block_rows(chip), :], preferred_element_type=jnp.float32
        )
        partial[k, :, :] = term if fresh else partial[k, :, :] + term

    for k in range(2):
        hide(k)
        for j in range(SUB):
            for way in range(2):
                hop_copy(way, k, 0, j).start()
    columns_copy.wait()
    for k in range(2):
        add_block(k, pair, True)

    def source_of(way, step):
        return lax.rem(z + chips - step - 1 if way == 0 else z + step + 1, half_ring)

    def hop(step, _):
        @pl.when(step < own_count)
        def _():
            forward(2, step)

        for k in range(2):
            for j in range(SUB):
                for way in range(2):
                    hop_arrival(way, k, step, j).wait_recv()

                    @pl.when(jnp.logical_or(step < reach - 2, k == way))
                    def _():
                        hop_copy(way, k, step + 1, j).start()

        for k in range(2):
            for way in range(2):
                add_block(k, source_of(way, step))
        return 0

    lax.fori_loop(0, reach - 1, hop, 0)
    for j in range(reach - 1, own_count):
        forward(2, j)
    for way in range(2):
        for j in range(SUB):
            hop_arrival(way, way, reach - 1, j).wait_recv()
    for k in range(2):
        add_block(k, source_of(k, reach - 1))

    def back_copy(step, core):
        other = lax.rem(t + step, experts)
        return pltpu.make_async_remote_copy(
            src_ref=column_out.at[other, rows_at(core), :],
            dst_ref=returned.at[t, c],
            send_sem=back_send.at[step, core],
            recv_sem=back_recv.at[t, c],
            device_id={"tp": other, "fs_1": core},
            device_id_type=MESH,
        )

    def back_arrival(step, core):
        other = lax.rem(t + step, experts)
        return pltpu.make_async_remote_copy(
            src_ref=column_out.at[other, rows_at(c), :],
            dst_ref=returned.at[other, core],
            send_sem=back_send.at[step, core],
            recv_sem=back_recv.at[other, core],
            device_id={"tp": other, "fs_1": core},
            device_id_type=MESH,
        )

    for e in range(experts):
        k, lane = e // (experts // 2), (e % (experts // 2)) * CAP
        column_out[e, :, :] = partial[k, :, lane : lane + CAP]
    for step in range(1, experts):
        for core in range(2):
            back_copy(step, core).start()
    back_copy(0, 1 - c).start()
    returned[t, c] = column_out[t, rows_at(c), :]
    back_arrival(0, 1 - c).wait_recv()
    for step in range(1, experts):
        for core in range(2):
            back_arrival(step, core).wait_recv()
    total = jnp.zeros((rows, token_count), jnp.float32)
    for e in range(experts):
        weight = jnp.where(first == e, route_weight[0:1, :], 0.0) + jnp.where(
            second == e, route_weight[1:2, :], 0.0
        )
        total = total + weight * jnp.dot(
            (returned[e, 0] + returned[e, 1]).astype(jnp.bfloat16),
            select[e, :, :],
            preferred_element_type=jnp.float32,
        )
    mixed_out[...] = total.astype(jnp.bfloat16)

    arrive(2)
    for m in range(3):

        @pl.when(active)
        def _():
            for k in range(3):
                mate_copy(m, k).wait_send()

            def sent(i, _):
                @pl.when(jnp.logical_not(is_mine(i)))
                def _():
                    ring_copy(m, i).wait_send()

                return 0

            lax.fori_loop(0, blocks, sent, 0)

        def passed(j, _):
            for step in range(1, groups):
                group_copy(m, j, step).wait_send()
            return 0

        lax.fori_loop(0, own_count, passed, 0)

    def hopped(step, _):
        for k in range(2):
            for way in range(2):

                @pl.when(jnp.logical_or(step < reach - 1, k == way))
                def _():
                    for j in range(SUB):
                        hop_copy(way, k, step, j).wait_send()

        return 0

    lax.fori_loop(0, reach, hopped, 0)
    for step in range(1, experts):
        token_copy(step).wait_send()
        for core in range(2):
            back_copy(step, core).wait_send()
    back_copy(0, 1 - c).wait_send()


def layer(groups, chips, experts, *operands):
    tokens, gate = operands[3], operands[4]
    rows, hidden = gate.shape
    units = hidden // chips
    width = rows * 2 * chips
    quads = chips // 2
    share = hidden // 4
    reach = chips // 4
    wide = experts * CAP // 2
    served = jax.ShapeDtypeStruct((units, width), jnp.bfloat16)
    dma = pltpu.SemaphoreType.DMA
    return pl.pallas_call(
        functools.partial(layer_kernel, groups, chips, experts),
        out_shape=(
            served,
            served,
            served,
            jax.ShapeDtypeStruct((rows, tokens.shape[0]), jnp.bfloat16),
        ),
        in_specs=[pl.BlockSpec(memory_space=pltpu.VMEM)] * 3
        + [pl.BlockSpec(memory_space=pltpu.HBM)] * 4,
        out_specs=[pl.BlockSpec(memory_space=pltpu.VMEM)] * 4,
        scratch_shapes=[
            pltpu.VMEM(tokens.shape, jnp.bfloat16),
            pltpu.VMEM((3, rows, hidden), jnp.float32),
            pltpu.VMEM((3, rows, hidden), jnp.bfloat16),
            pltpu.VMEM((3, 4 * rows, share), jnp.bfloat16),
            pltpu.VMEM((3, share, 4 * rows), jnp.bfloat16),
            pltpu.VMEM((experts, CAP, tokens.shape[0]), jnp.bfloat16),
            pltpu.VMEM((experts, CAP, width), jnp.bfloat16),
            pltpu.VMEM((experts, CAP, width), jnp.bfloat16),
            pltpu.VMEM((2, chips // 2, rows, units), jnp.bfloat16),
            pltpu.VMEM((chips // 2, 2 * rows, units), jnp.bfloat16),
            pltpu.VMEM((2, hidden // 2, wide), jnp.bfloat16),
            pltpu.VMEM((2, 2 * rows, wide), jnp.float32),
            pltpu.VMEM((experts, 2 * rows, CAP), jnp.float32),
            pltpu.VMEM((experts, 2, rows, CAP), jnp.float32),
            dma((3, 3)),
            dma((3, 4)),
            dma((3, share // units)),
            dma((3, quads)),
            dma((3, quads // groups, groups - 1)),
            dma((experts - 1,)),
            dma((experts,)),
            dma((1,)),
            dma((1,)),
            dma((2, 2, reach, SUB)),
            dma((2, 2, reach, SUB)),
            dma((experts, 2)),
            dma((experts, 2)),
            dma((4,)),
            pltpu.SemaphoreType.REGULAR,
        ],
        compiler_params=pltpu.CompilerParams(
            collective_id=0, has_side_effects=True, vmem_limit_bytes=52736 * 1024
        ),
        name="layer",
    )(*operands)


def store_kernel(*refs):
    count = len(refs) // 2
    sem = refs[-1]
    copies = [
        pltpu.make_async_copy(refs[i], refs[count + i], sem.at[i]) for i in range(count)
    ]
    for copy in copies:
        copy.start()
    for copy in copies:
        copy.wait()


def stored(arrays):
    return pl.pallas_call(
        store_kernel,
        out_shape=tuple(jax.ShapeDtypeStruct(x.shape, x.dtype) for x in arrays),
        in_specs=[pl.BlockSpec(memory_space=pltpu.VMEM)] * len(arrays),
        out_specs=[pl.BlockSpec(memory_space=pltpu.HBM)] * len(arrays),
        scratch_shapes=[pltpu.SemaphoreType.DMA((len(arrays),))],
        compiler_params=pltpu.CompilerParams(vmem_limit_bytes=4 * 1024 * 1024),
        name="store",
    )(*arrays)


def shards(tokens, routes, route_weight, norm_gain, gate_train, up_train, down_train):
    results = layer(
        lax.axis_size("grp"),
        lax.axis_size("fs_0"),
        lax.axis_size("tp"),
        routes.T,
        route_weight.T,
        norm_gain[None, :],
        tokens,
        gate_train[0],
        up_train[0],
        down_train[0].T,
    )
    gate_new, up_new, down_new, mixed = stored(results)
    return (gate_new.T[None], up_new.T[None], down_new[None], mixed.T)


def solution(mesh):
    cores = 2
    split = Mesh(
        mesh.devices.reshape(
            mesh.shape["grp"], mesh.shape["fs"] // cores, cores, mesh.shape["tp"]
        ),
        ("grp", "fs_0", "fs_1", "tp"),
    )
    placed = (
        P(("grp", "tp"), None),
        P(("grp", "tp"), None),
        P(("grp", "tp"), None),
        P(FS),
        P("tp", FS, None),
        P("tp", FS, None),
        P("tp", None, FS),
    )
    return jax.shard_map(
        shards,
        mesh=split,
        in_specs=placed,
        out_specs=(
            P(("grp", "tp"), None, FS),
            P(("grp", "tp"), None, FS),
            P(("grp", "tp"), FS, None),
            P(("grp", "tp"), FS),
        ),
        check_vma=False,
    )
```

```python
import functools

import jax
import jax.numpy as jnp
from jax import lax
from jax.experimental import pallas as pl
from jax.experimental.pallas import tpu as pltpu
from jax.sharding import Mesh
from jax.sharding import PartitionSpec as P

CAP = 128
LANES = 128
FS = ("fs_0", "fs_1")
MESH = pl.DeviceIdType.MESH
SUB = 2
NT = (((1,), (1,)), ((), ()))


def layer_kernel(
    groups,
    chips,
    experts,
    routes,
    route_weight,
    gain,
    tokens_far,
    gate_far,
    up_far,
    down_far,
    gate_out,
    up_out,
    down_out,
    mixed_out,
    tokens,
    full,
    low,
    rows_buf,
    tile_buf,
    select,
    outgoing,
    arrived,
    split_down,
    my_down,
    hidden_all,
    partial,
    column_out,
    returned,
    quad_send,
    quad_recv,
    ring_send,
    unit_recv,
    group_send,
    token_send,
    token_recv,
    core_send,
    core_recv,
    hop_send,
    hop_recv,
    back_send,
    back_recv,
    read_sem,
    ready,
):
    g = lax.axis_index("grp")
    z = lax.axis_index("fs_0")
    c = lax.axis_index("fs_1")
    t = lax.axis_index("tp")
    quads = chips // 2
    half_ring = chips // 2
    rows, hidden = gate_far.shape
    units = gate_out.shape[0]
    spread = groups // 2
    share = hidden // 4
    blocks = share // units
    own_count = quads // groups
    slots = experts * CAP
    q = z // 2
    odd = lax.rem(z, 2)
    me = 2 * odd + c
    half = lax.rem(g + q // spread, 2)
    active = lax.rem(q, spread) == g // 2
    pair = lax.rem(z, half_ring)
    my_block = 2 * pair + c
    my_half = my_block // (2 * blocks)
    my_source_core = lax.rem(my_block, 2 * blocks) // blocks
    parity = lax.rem(my_half + g, 2)
    own = jnp.logical_and(active, jnp.logical_and(half == my_half, c == my_source_core))
    outputs = (gate_out, up_out, down_out)
    reach = half_ring // 2

    def at(chip, core):
        return {"fs_0": chip, "fs_1": core}

    def own_quad(j):
        return spread * (2 * j + parity) + g // 2

    def listed(m, n):
        if m == 1:
            return jnp.where(lax.rem(q // (2 * spread), 2) == 1, blocks - 1 - n, n)
        return lax.rem(n + c * (blocks // 2), blocks)

    def expected_quad(m, n):
        if m == 1 and own_count > 1:
            early = lax.rem(my_block, blocks) >= blocks // 2
            wanted = own_count // 2
            first_half = n < wanted
            odd_turn = jnp.logical_xor(early, jnp.logical_not(first_half))
            within = jnp.where(first_half, n, n - wanted)
            return own_quad(2 * within + jnp.where(odd_turn, 1, 0))
        return own_quad(n)

    def target(i):
        chip = half * blocks + c * (blocks // 2) + i // 2
        right = lax.rem(chip - z + 2 * chips, half_ring)
        left = lax.rem(z - chip + 2 * chips, half_ring)
        chip = jnp.where(odd == 1, z + right, z - left + chips)
        return lax.rem(chip, chips), lax.rem(i, 2)

    def place(index):
        return pl.ds(pl.multiple_of(index * LANES, LANES), LANES)

    def block_rows(index):
        return pl.ds(pl.multiple_of(index * units, 16), units)

    def rows_at(index):
        return pl.ds(pl.multiple_of(index * rows, rows), rows)

    quad_mates = ((z + 1 - 2 * odd, c), (z, 1 - c), (z + 1 - 2 * odd, 1 - c))
    next_chip = lax.rem(z + 1, chips)
    last_chip = lax.rem(z + chips - 1, chips)

    reads = [
        pltpu.make_async_copy(far, full.at[m], read_sem.at[m])
        for m, far in enumerate((gate_far, up_far, down_far))
    ]
    reads.append(pltpu.make_async_copy(tokens_far, tokens, read_sem.at[3]))
    for read in reads:
        read.start()

    barrier = pltpu.get_barrier_semaphore()

    def greet_device(where):
        pl.semaphore_signal(barrier, inc=1, device_id=where, device_id_type=MESH)

    for k in range(reach // 2):
        for core in range(2):
            greet_device(at(lax.rem(z + chips - (2 * k + 1 + odd), chips), core))
            greet_device(at(lax.rem(z + 2 * k + 2 - odd, chips), core))
    ahead = lax.rem(jnp.where(odd == 1, z + reach, z + chips - reach), chips)
    behind = lax.rem(jnp.where(odd == 1, z + chips - reach, z + reach), chips)
    greet_device(at(ahead, c))
    for chip, core in quad_mates:
        greet_device(at(chip, core))
    for step in range(1, groups):
        greet_device({"grp": lax.rem(g + step, groups)})
    for step in range(1, experts):
        for core in range(2):
            greet_device({"tp": lax.rem(t + step, experts), "fs_1": core})
    greet_device(at(next_chip, c))
    greet_device(at(last_chip, c))

    eye = lax.broadcasted_iota(jnp.int32, (rows, rows), 0) == lax.broadcasted_iota(
        jnp.int32, (rows, rows), 1
    )
    gain_column = jnp.sum(jnp.where(eye, gain[...], 0.0), axis=1, keepdims=True)
    for m in range(2):
        reads[m].wait()
        low[m, :, :] = (full[m] * gain_column).astype(jnp.bfloat16)
    reads[2].wait()
    low[2, :, :] = full[2].astype(jnp.bfloat16)

    pl.semaphore_wait(barrier, groups - 1 + 3 + 2 * (experts - 1) + 2 + 2 * reach + 1)

    def lanes_for(core):
        return pl.ds(pl.multiple_of((2 * half + core) * share, LANES), share)

    def mate_copy(m, k):
        chip, core = quad_mates[k]
        return pltpu.make_async_remote_copy(
            src_ref=low.at[m, :, lanes_for(core)],
            dst_ref=rows_buf.at[m, rows_at(me), :],
            send_sem=quad_send.at[m, k],
            recv_sem=quad_recv.at[m, me],
            device_id=at(chip, core),
            device_id_type=MESH,
        )

    def ring_copy(m, i):
        chip, core = target(i)
        return pltpu.make_async_remote_copy(
            src_ref=tile_buf.at[m, block_rows(i), :],
            dst_ref=outputs[m].at[:, place(q)],
            send_sem=ring_send.at[m, i],
            recv_sem=unit_recv.at[m, q],
            device_id=at(chip, core),
            device_id_type=MESH,
        )

    def group_copy(m, j, step):
        other = expected_quad(m, j)
        return pltpu.make_async_remote_copy(
            src_ref=outputs[m].at[:, place(other)],
            dst_ref=outputs[m].at[:, place(other)],
            send_sem=group_send.at[m, j, step - 1],
            recv_sem=unit_recv.at[m, other],
            device_id={"grp": lax.rem(g + step, groups)},
            device_id_type=MESH,
        )

    def unit_arrival(m, index):
        return pltpu.make_async_remote_copy(
            src_ref=outputs[m].at[:, place(index)],
            dst_ref=outputs[m].at[:, place(index)],
            send_sem=group_send.at[m, 0, 0],
            recv_sem=unit_recv.at[m, index],
            device_id={"grp": lax.rem(g + 1, groups)},
            device_id_type=MESH,
        )

    def is_near(i):
        chip, _ = target(i)
        away = lax.rem(jnp.where(odd == 1, chip - z, z - chip) + chips, chips)
        return away <= reach

    def is_mine(i):
        chip, core = target(i)
        return jnp.logical_and(chip == z, core == c)

    def send_tile(m, i):
        mine = is_mine(i)

        @pl.when(mine)
        def _():
            outputs[m][:, place(q)] = tile_buf[m, block_rows(i), :]

        @pl.when(jnp.logical_not(mine))
        def _():
            ring_copy(m, i).start()

    def token_copy(step):
        other = lax.rem(t + step, experts)
        return pltpu.make_async_remote_copy(
            src_ref=outgoing.at[other],
            dst_ref=arrived.at[t],
            send_sem=token_send.at[step - 1],
            recv_sem=token_recv.at[t],
            device_id={"tp": other},
            device_id_type=MESH,
        )

    def token_arrival(step):
        other = lax.rem(t + step, experts)
        return pltpu.make_async_remote_copy(
            src_ref=outgoing.at[other],
            dst_ref=arrived.at[other],
            send_sem=token_send.at[step - 1],
            recv_sem=token_recv.at[other],
            device_id={"tp": other},
            device_id_type=MESH,
        )

    @pl.when(active)
    def _():
        for m in range(2):
            for k in range(3):
                mate_copy(m, k).start()

    pl.semaphore_signal(ready, inc=1, device_id=at(behind, c), device_id_type=MESH)

    token_count, width = tokens.shape
    first = routes[0:1, :]
    second = routes[1:2, :]
    expert_row = lax.broadcasted_iota(jnp.int32, (8, token_count), 0)
    named = jnp.logical_or(first == expert_row, second == expert_row)
    before = (
        lax.broadcasted_iota(jnp.int32, (token_count, token_count), 0)
        < lax.broadcasted_iota(jnp.int32, (token_count, token_count), 1)
    )
    rank = jnp.dot(
        jnp.where(named, 1.0, 0.0).astype(jnp.bfloat16),
        jnp.where(before, 1.0, 0.0).astype(jnp.bfloat16),
        preferred_element_type=jnp.float32,
    )
    slot = lax.broadcasted_iota(jnp.int32, (CAP, token_count), 0).astype(jnp.float32)
    reads[3].wait()
    tok_float = tokens[...].astype(jnp.float32)
    normed = (
        tok_float * lax.rsqrt(jnp.mean(tok_float * tok_float, axis=-1, keepdims=True) + 1e-06)
    ).astype(jnp.bfloat16)
    for e in range(experts):
        chosen = jnp.logical_or(first == e, second == e)
        hot = jnp.logical_and(slot == rank[e : e + 1, :], chosen)
        select[e, :, :] = jnp.where(hot, 1.0, 0.0).astype(jnp.bfloat16)
        outgoing[e, :, :] = jnp.dot(
            select[e, :, :], normed, preferred_element_type=jnp.float32
        ).astype(jnp.bfloat16)

    for step in range(1, experts):
        token_copy(step).start()
    arrived[t] = outgoing[t]

    @pl.when(active)
    def _():
        for m in range(3):
            rows_buf[m, rows_at(me), :] = low[m, :, lanes_for(c)]
            for k in range(3):
                chip_back, core_back = quad_mates[k]
                source = 2 * lax.rem(chip_back, 2) + core_back
                pltpu.make_async_remote_copy(
                    src_ref=low.at[m, :, lanes_for(c)],
                    dst_ref=rows_buf.at[m, rows_at(source), :],
                    send_sem=quad_send.at[m, k],
                    recv_sem=quad_recv.at[m, source],
                    device_id=at(chip_back, core_back),
                    device_id_type=MESH,
                ).wait_recv()
            tile_buf[m, :, :] = rows_buf[m, :, :].T

            def send(n, _):
                send_tile(m, listed(m, n))
                return 0

            def send_if(near, n, _):
                @pl.when(is_near(n) == near)
                def _():
                    send_tile(m, n)

                return 0

            if m == 0:
                pl.semaphore_wait(ready, 1)
            lax.fori_loop(0, blocks, send, 0)
            if m == 0:
                for k in range(3):
                    mate_copy(2, k).start()

    @pl.when(jnp.logical_not(active))
    def _():
        pl.semaphore_wait(ready, 1)


    for k in range(half_ring):
        for p in range(2):
            start = (2 * k + p) * units
            split_down[p, k, :, :] = low[2, :, start : start + units]
    for k in range(half_ring):
        my_down[k, rows_at(c), :] = split_down[c, k]
    columns_copy = pltpu.make_async_remote_copy(
        src_ref=split_down.at[1 - c],
        dst_ref=my_down.at[:, rows_at(c), :],
        send_sem=core_send.at[0],
        recv_sem=core_recv.at[0],
        device_id=at(z, 1 - c),
        device_id_type=MESH,
    )
    columns_copy.start()

    def forward(m, j):
        other = expected_quad(m, j)

        @pl.when(jnp.logical_not(jnp.logical_and(own, other == q)))
        def _():
            unit_arrival(m, other).wait_recv()

        for step in range(1, groups):
            group_copy(m, j, step).start()

    def arrive(m):
        def body(index, _):
            here = jnp.logical_and(
                lax.rem(index, spread) == g // 2, lax.rem(index // spread, 2) == parity
            )

            @pl.when(jnp.logical_not(here))
            def _():
                unit_arrival(m, index).wait_recv()

            return 0

        lax.fori_loop(0, quads, body, 0)

    for m in range(2):

        def body(j, _):
            forward(m, j)
            return 0

        lax.fori_loop(0, own_count, body, 0)
    for m in range(2):
        arrive(m)
    for step in range(1, experts):
        token_arrival(step).wait_recv()

    wide = slots // 2

    def hide(k):
        own_tokens = arrived[k * (experts // 2) : (k + 1) * (experts // 2)].reshape(wide, width)
        gated = lax.dot_general(gate_out[...], own_tokens, NT, preferred_element_type=jnp.float32)
        lifted = lax.dot_general(up_out[...], own_tokens, NT, preferred_element_type=jnp.float32)
        hidden_all[k, block_rows(pair), :] = (
            gated * (1.0 / (1.0 + jnp.exp(-gated))) * lifted
        ).astype(jnp.bfloat16)

    part = wide // SUB

    def hop_copy(way, k, step, j):
        chip = lax.rem(z + chips - step if way == 0 else z + step, half_ring)
        return pltpu.make_async_remote_copy(
            src_ref=hidden_all.at[k, block_rows(chip), pl.ds(j * part, part)],
            dst_ref=hidden_all.at[k, block_rows(chip), pl.ds(j * part, part)],
            send_sem=hop_send.at[way, k, step, j],
            recv_sem=hop_recv.at[way, k, step, j],
            device_id=at(next_chip if way == 0 else last_chip, c),
            device_id_type=MESH,
        )

    def hop_arrival(way, k, step, j):
        chip = lax.rem(z + chips - step - 1 if way == 0 else z + step + 1, half_ring)
        return pltpu.make_async_remote_copy(
            src_ref=hidden_all.at[k, block_rows(chip), pl.ds(j * part, part)],
            dst_ref=hidden_all.at[k, block_rows(chip), pl.ds(j * part, part)],
            send_sem=hop_send.at[way, k, step, j],
            recv_sem=hop_recv.at[way, k, step, j],
            device_id=at(last_chip if way == 0 else next_chip, c),
            device_id_type=MESH,
        )

    def add_block(k, chip, fresh=False):
        term = jnp.dot(
            my_down[chip], hidden_all[k, block_rows(chip), :], preferred_element_type=jnp.float32
        )
        partial[k, :, :] = term if fresh else partial[k, :, :] + term

    for k in range(2):
        hide(k)
        for j in range(SUB):
            for way in range(2):
                hop_copy(way, k, 0, j).start()
    columns_copy.wait()
    for k in range(2):
        add_block(k, pair, True)

    def source_of(way, step):
        return lax.rem(z + chips - step - 1 if way == 0 else z + step + 1, half_ring)

    def hop(step, _):
        skipped = reach - 1 - (own_count + 1) // 2

        @pl.when(step >= skipped)
        def _():
            forward(2, 2 * (step - skipped))
            if own_count > 1:
                forward(2, 2 * (step - skipped) + 1)

        for long in (True, False):
            for j in range(SUB):
                for way in range(2):
                    k = way if long else 1 - way
                    hop_arrival(way, k, step, j).wait_recv()
                    if long:
                        hop_copy(way, k, step + 1, j).start()
                    else:

                        @pl.when(step < reach - 2)
                        def _():
                            hop_copy(way, k, step + 1, j).start()

        for k in range(2):
            for way in range(2):
                add_block(k, source_of(way, step))
        return 0

    lax.fori_loop(0, reach - 1, hop, 0)
    for way in range(2):
        for j in range(SUB):
            hop_arrival(way, way, reach - 1, j).wait_recv()
    for k in range(2):
        add_block(k, source_of(k, reach - 1))

    def back_copy(step, core):
        other = lax.rem(t + step, experts)
        return pltpu.make_async_remote_copy(
            src_ref=column_out.at[other, rows_at(core), :],
            dst_ref=returned.at[t, c],
            send_sem=back_send.at[step, core],
            recv_sem=back_recv.at[t, c],
            device_id={"tp": other, "fs_1": core},
            device_id_type=MESH,
        )

    def back_arrival(step, core):
        other = lax.rem(t + step, experts)
        return pltpu.make_async_remote_copy(
            src_ref=column_out.at[other, rows_at(c), :],
            dst_ref=returned.at[other, core],
            send_sem=back_send.at[step, core],
            recv_sem=back_recv.at[other, core],
            device_id={"tp": other, "fs_1": core},
            device_id_type=MESH,
        )

    for e in range(experts):
        k, lane = e // (experts // 2), (e % (experts // 2)) * CAP
        column_out[e, :, :] = partial[k, :, lane : lane + CAP]
    for step in range(1, experts):
        for core in range(2):
            back_copy(step, core).start()
    back_copy(0, 1 - c).start()
    returned[t, c] = column_out[t, rows_at(c), :]
    back_arrival(0, 1 - c).wait_recv()
    for step in range(1, experts):
        for core in range(2):
            back_arrival(step, core).wait_recv()
    total = jnp.zeros((rows, token_count), jnp.float32)
    for e in range(experts):
        weight = jnp.where(first == e, route_weight[0:1, :], 0.0) + jnp.where(
            second == e, route_weight[1:2, :], 0.0
        )
        total = total + weight * jnp.dot(
            (returned[e, 0] + returned[e, 1]).astype(jnp.bfloat16),
            select[e, :, :],
            preferred_element_type=jnp.float32,
        )
    mixed_out[...] = total.astype(jnp.bfloat16)

    arrive(2)
    for m in range(3):

        @pl.when(active)
        def _():
            for k in range(3):
                mate_copy(m, k).wait_send()

            def sent(i, _):
                @pl.when(jnp.logical_not(is_mine(i)))
                def _():
                    ring_copy(m, i).wait_send()

                return 0

            lax.fori_loop(0, blocks, sent, 0)

        def passed(j, _):
            for step in range(1, groups):
                group_copy(m, j, step).wait_send()
            return 0

        lax.fori_loop(0, own_count, passed, 0)

    def hopped(step, _):
        for k in range(2):
            for way in range(2):

                @pl.when(jnp.logical_or(step < reach - 1, k == way))
                def _():
                    for j in range(SUB):
                        hop_copy(way, k, step, j).wait_send()

        return 0

    lax.fori_loop(0, reach, hopped, 0)
    for step in range(1, experts):
        token_copy(step).wait_send()
        for core in range(2):
            back_copy(step, core).wait_send()
    back_copy(0, 1 - c).wait_send()


def layer(groups, chips, experts, *operands):
    tokens, gate = operands[3], operands[4]
    rows, hidden = gate.shape
    units = hidden // chips
    width = rows * 2 * chips
    quads = chips // 2
    share = hidden // 4
    reach = chips // 4
    wide = experts * CAP // 2
    served = jax.ShapeDtypeStruct((units, width), jnp.bfloat16)
    dma = pltpu.SemaphoreType.DMA
    return pl.pallas_call(
        functools.partial(layer_kernel, groups, chips, experts),
        out_shape=(
            served,
            served,
            served,
            jax.ShapeDtypeStruct((rows, tokens.shape[0]), jnp.bfloat16),
        ),
        in_specs=[pl.BlockSpec(memory_space=pltpu.VMEM)] * 3
        + [pl.BlockSpec(memory_space=pltpu.HBM)] * 4,
        out_specs=[pl.BlockSpec(memory_space=pltpu.VMEM)] * 4,
        scratch_shapes=[
            pltpu.VMEM(tokens.shape, jnp.bfloat16),
            pltpu.VMEM((3, rows, hidden), jnp.float32),
            pltpu.VMEM((3, rows, hidden), jnp.bfloat16),
            pltpu.VMEM((3, 4 * rows, share), jnp.bfloat16),
            pltpu.VMEM((3, share, 4 * rows), jnp.bfloat16),
            pltpu.VMEM((experts, CAP, tokens.shape[0]), jnp.bfloat16),
            pltpu.VMEM((experts, CAP, width), jnp.bfloat16),
            pltpu.VMEM((experts, CAP, width), jnp.bfloat16),
            pltpu.VMEM((2, chips // 2, rows, units), jnp.bfloat16),
            pltpu.VMEM((chips // 2, 2 * rows, units), jnp.bfloat16),
            pltpu.VMEM((2, hidden // 2, wide), jnp.bfloat16),
            pltpu.VMEM((2, 2 * rows, wide), jnp.float32),
            pltpu.VMEM((experts, 2 * rows, CAP), jnp.float32),
            pltpu.VMEM((experts, 2, rows, CAP), jnp.float32),
            dma((3, 3)),
            dma((3, 4)),
            dma((3, share // units)),
            dma((3, quads)),
            dma((3, quads // groups, groups - 1)),
            dma((experts - 1,)),
            dma((experts,)),
            dma((1,)),
            dma((1,)),
            dma((2, 2, reach, SUB)),
            dma((2, 2, reach, SUB)),
            dma((experts, 2)),
            dma((experts, 2)),
            dma((4,)),
            pltpu.SemaphoreType.REGULAR,
        ],
        compiler_params=pltpu.CompilerParams(
            collective_id=0, has_side_effects=True, vmem_limit_bytes=52736 * 1024
        ),
        name="layer",
    )(*operands)


def store_kernel(*refs):
    count = len(refs) // 2
    sem = refs[-1]
    copies = [
        pltpu.make_async_copy(refs[i], refs[count + i], sem.at[i]) for i in range(count)
    ]
    for copy in copies:
        copy.start()
    for copy in copies:
        copy.wait()


def stored(arrays):
    return pl.pallas_call(
        store_kernel,
        out_shape=tuple(jax.ShapeDtypeStruct(x.shape, x.dtype) for x in arrays),
        in_specs=[pl.BlockSpec(memory_space=pltpu.VMEM)] * len(arrays),
        out_specs=[pl.BlockSpec(memory_space=pltpu.HBM)] * len(arrays),
        scratch_shapes=[pltpu.SemaphoreType.DMA((len(arrays),))],
        compiler_params=pltpu.CompilerParams(vmem_limit_bytes=4 * 1024 * 1024),
        name="store",
    )(*arrays)


def shards(tokens, routes, route_weight, norm_gain, gate_train, up_train, down_train):
    results = layer(
        lax.axis_size("grp"),
        lax.axis_size("fs_0"),
        lax.axis_size("tp"),
        routes.T,
        route_weight.T,
        norm_gain[None, :],
        tokens,
        gate_train[0],
        up_train[0],
        down_train[0].T,
    )
    gate_new, up_new, down_new, mixed = stored(results)
    return (gate_new.T[None], up_new.T[None], down_new[None], mixed.T)


def solution(mesh):
    cores = 2
    split = Mesh(
        mesh.devices.reshape(
            mesh.shape["grp"], mesh.shape["fs"] // cores, cores, mesh.shape["tp"]
        ),
        ("grp", "fs_0", "fs_1", "tp"),
    )
    placed = (
        P(("grp", "tp"), None),
        P(("grp", "tp"), None),
        P(("grp", "tp"), None),
        P(FS),
        P("tp", FS, None),
        P("tp", FS, None),
        P("tp", None, FS),
    )
    return jax.shard_map(
        shards,
        mesh=split,
        in_specs=placed,
        out_specs=(
            P(("grp", "tp"), None, FS),
            P(("grp", "tp"), None, FS),
            P(("grp", "tp"), FS, None),
            P(("grp", "tp"), FS),
        ),
        check_vma=False,
    )
```
